512 devices in a mesh: grp: 2 (over y), ep: 16 (over z), tp: 16 (over x, core).
Axes of the slice: x: 8, y: 2, z: 16, core: 2. Of those that a mesh axis runs over, the one named last changes fastest.
The devices are a block of a 8x16x16 slice.
Arguments:
- tokens: bfloat16 [1024, 2048], P(('grp', 'ep'), 'tp'), parts along dimension 0, may hold values from -6 to 6
- gain: float32 [2048], replicated, may hold values from 0.1 to 1.9
- routes: int32 [1024, 4], P(('grp', 'ep')), parts along dimension 0, may hold values from 0 to 15, all different within a row; in each aligned block of 32 rows (0 to 31, 32 to 63, ...) at most 16 rows name the same one
- weights: float32 [1024, 4], P(('grp', 'ep')), parts along dimension 0, may hold values from 0.05 to 1
- w_gate: bfloat16 [16, 2048, 6144], P('ep', None, 'tp'), may hold values from -0.125 to 0.125
- w_up: bfloat16 [16, 2048, 6144], P('ep', None, 'tp'), may hold values from -0.125 to 0.125
- w_down: bfloat16 [16, 6144, 2048], P('ep', 'tp'), may hold values from -0.078125 to 0.078125
Outputs:
- mixed: bfloat16 [1024, 2048], P(('grp', 'ep'), 'tp'), parts along dimension 0
The draws below stay inside these ranges and needn't reach their ends.
There are 2 independent parts, one for each index of `grp`. The reference program is written for one: setup_inputs(seed, part) draws one part's arguments, and reference() takes and returns one part's arrays. A program takes and returns all parts, laid end to end along the dimension named above; an argument that names none is the same for every part. Nothing has to cross between parts.
Inputs may be any that keep to these rules, and one draw needn't show every extreme that they name: `routes`: each row names 4 different experts. Among the rows of one device no expert is named by more than 16 rows, a bound that some block reaches.
All inputs are finite; a program needn't handle non-finite values.
Results may differ from the reference program's by a relative error of at most 0.019.
Values may be sent and summed in bfloat16 or wider, within the bound.
A program may use at most 64 MiB of HBM per device.

```python
import math
import jax
import jax.numpy as jnp
import numpy as np
from jax import lax

D = 2048
FF = 6144
TOP = 4
TOK_DEV = 32
EXPERTS = 16
CAP = 16
TOKENS = 512
N_EP = 16
N_TP = 16


def levels(own_key, shape, pieces, smallest, high):
    level = 1.0
    for axis_at, blocks in pieces:
        steps = jax.random.uniform(jax.random.fold_in(jax.random.fold_in(own_key, 6), axis_at), (blocks,), jnp.float32, smallest / len(pieces), high / len(pieces))
        level = level * jnp.repeat(jnp.exp(steps), shape[axis_at] // blocks).reshape((-1,) + (1,) * (len(shape) - 1 - axis_at))
    return level


def routed_block(rng, own, number, rows, number_of, top, most, skew):
    sequence = jax.random.permutation(rng, number_of)
    heavy_load, ordinary = portions_of(number_of, rows * top, most, skew, True), portions_of(number_of, rows * top, most, skew, False)
    places = jnp.arange(number_of)

    def named(tallies, offset_by):
        used = int((tallies > 0).sum())
        fixed = max(1, used // 4)
        moved = fixed + (places - fixed + offset_by * (used - fixed)) % max(1, number_of - fixed)
        return jnp.zeros((number_of,), jnp.int32).at[sequence[jnp.where(places < fixed, places, moved)]].set(jnp.asarray(tallies, jnp.int32))

    tallies = jnp.where(number % 4 == 0, named(heavy_load, number // 4), named(ordinary, number - number // 4 - 1))
    mixed = jax.random.permutation(jax.random.fold_in(own, 3), number_of)
    giver, receiver = mixed[0:number_of // 2 * 2:2], mixed[1:number_of // 2 * 2:2]
    slack = jnp.minimum(tallies[giver] - 1, most - tallies[receiver]) // 2
    slack = jnp.where((giver == sequence[0]) | (receiver == sequence[0]) | (tallies[receiver] == 0), 0, jnp.maximum(slack, 0))
    moved = jax.random.randint(jax.random.fold_in(own, 4), (number_of // 2,), 0, 1 << 20) % (slack + 1)
    tallies = tallies.at[giver].add(-moved).at[receiver].add(moved)
    items = jnp.searchsorted(jnp.cumsum(tallies), jnp.arange(rows * top), side="right").astype(jnp.int32)
    listing = items.reshape(top, rows).T
    listing = listing[jax.random.permutation(jax.random.fold_in(own, 1), rows)]
    offset_by = jax.random.randint(jax.random.fold_in(own, 2), (rows, 1), 0, top)
    return jnp.take_along_axis(listing, (jnp.arange(top)[None, :] + offset_by) % top, axis=1)


def portions_of(count, total, most, lean, full):
    weights = [(1 << 20) // math.isqrt(grade ** lean) + 1 for grade in range(1, count + 1)]
    largest = most if full else min(most, max(-(-total // count), total * weights[0] // sum(weights)))
    least = 1 if total - largest >= count - 1 else 0
    given, surplus = [largest] + [least] * (count - 1), total - largest - least * (count - 1)
    while surplus > 0:
        free = [i for i in range(1, count) if given[i] < largest] or [i for i in range(1, count) if given[i] < most]
        whole, budget = sum([weights[i] for i in free]), surplus
        for i in free:
            extra = min(most - given[i], max(1, budget * weights[i] // whole), surplus)
            given[i] = given[i] + extra
            surplus = surplus - extra
    return np.array(given)


def noise(rng, shape, scale, limit, split=(), held_as=jnp.bfloat16):
    result = scale * jax.random.normal(rng, shape, jnp.float32)
    if split:
        result = result * levels(rng, shape, split, -0.22, 0.18)
    return jnp.clip(result, -limit, limit).astype(held_as)


def setup_inputs(seed: int = 0, part: int = 0) -> dict:
    seeds = jax.random.split(jax.random.key(seed), 8)
    own_keys = jax.random.split(jax.random.fold_in(seeds[7], part), 8)
    tokens = noise(own_keys[0], (TOKENS, D), 1.0, 6.0, ((0, 16), (1, 16)))
    gain = jnp.clip(1.0 + 0.18 * jax.random.normal(seeds[1], (D,), jnp.float32), 0.1, 1.9)
    routes_keys = jax.random.split(jax.random.fold_in(own_keys[2], 1), TOKENS // TOK_DEV)
    routes_turns = jax.random.permutation(jax.random.fold_in(own_keys[2], 3), TOKENS // TOK_DEV)
    routes = jax.vmap(lambda own, number: routed_block(jax.random.fold_in(own_keys[2], 2), own, number, TOK_DEV, EXPERTS, TOP, CAP, 2))(routes_keys, routes_turns).reshape((TOKENS, TOP))
    weights = jnp.clip(jnp.exp(math.log(1.0) - 2.9957323 * jax.random.uniform(own_keys[3], (TOKENS, TOP), jnp.float32) ** levels(own_keys[3], (TOKENS, TOP), ((0, 16),), -0.2, 0.2)), 0.05, 1.0)
    w_gate = noise(seeds[4], (EXPERTS, D, FF), D ** -0.5, 0.125, ((0, 16), (2, 16)))
    w_up = noise(seeds[5], (EXPERTS, D, FF), D ** -0.5, 0.125, ((0, 16), (2, 16)))
    w_down = noise(seeds[6], (EXPERTS, FF, D), FF ** -0.5, 0.078125, ((0, 16), (1, 16)))
    return {"tokens": tokens, "gain": gain, "routes": routes, "weights": weights, "w_gate": w_gate, "w_up": w_up, "w_down": w_down}


epsilon = 1e-05

def normalize(values, gain):
    values = values.astype(jnp.float32)
    average = lax.optimization_barrier(jnp.mean(values, axis=1, keepdims=True))
    spread = lax.optimization_barrier(jnp.mean(jnp.square(values - average), axis=1, keepdims=True))
    return ((values - average) * lax.rsqrt(spread + epsilon) * gain).astype(jnp.bfloat16)

def reference(tokens, gain, routes, weights, w_gate, w_up, w_down):
    normed = normalize(tokens, gain)
    pair_count = TOKENS * TOP
    pair_expert = routes.reshape(-1).astype(jnp.int32)
    member = (pair_expert[:, None] == jnp.arange(EXPERTS, dtype=jnp.int32)[None, :]).astype(jnp.int32)
    earlier = jnp.cumsum(member, axis=0) - member
    room = N_EP * CAP
    position = (pair_expert * room + lax.optimization_barrier(jnp.sum(earlier * member, axis=1))).astype(jnp.int32)
    owner = jnp.full((EXPERTS * room,), TOKENS, jnp.int32)
    owner = owner.at[position].set(jnp.arange(pair_count, dtype=jnp.int32) // TOP)
    padded = jnp.concatenate([normed, jnp.zeros((1, D), jnp.bfloat16)], axis=0)
    block_width = FF // N_TP

    def expert(operands):
        index, gate_w, up_w, down_w = operands
        chosen = padded[index]
        gate_val = jnp.dot(chosen, gate_w, preferred_element_type=jnp.float32)
        up_val = jnp.dot(chosen, up_w, preferred_element_type=jnp.float32)
        hidden = (jax.nn.silu(gate_val) * up_val).astype(jnp.bfloat16)
        hidden_blocks = hidden.reshape(room, N_TP, block_width)
        down_blocks = down_w.reshape(N_TP, block_width, D)

        def one_block(carry, block):
            part = jnp.dot(block[0], block[1], preferred_element_type=jnp.float32).astype(jnp.bfloat16)
            return (carry + part.astype(jnp.float32), None)
        total, unused = lax.scan(one_block, jnp.zeros((room, D), jnp.float32), (jnp.swapaxes(hidden_blocks, 0, 1), down_blocks))
        return total.astype(jnp.bfloat16)
    results = lax.map(expert, (owner.reshape(EXPERTS, room), w_gate, w_up, w_down))
    results = results.reshape(EXPERTS * room, D)
    picked = results[position].reshape(TOKENS, TOP, D).astype(jnp.float32)
    return lax.optimization_barrier(jnp.sum(picked * weights[:, :, None], axis=1)).astype(jnp.bfloat16)
```

```python
import functools

import jax
import jax.numpy as jnp
from jax import lax
from jax.experimental import pallas as pl
from jax.experimental.pallas import tpu as pltpu
from jax.sharding import PartitionSpec as P

MESH = pl.DeviceIdType.MESH
epsilon = 1e-05
CHIPS = 8
CHUNKS = 2


def ring_offsets(count):
    offsets = [0]
    for distance in range(1, count // 2):
        offsets += [distance, -distance]
    return offsets + [count // 2]


def kernel(
    n_ep, cap,
    tok_hbm, gain_hbm, routes_hbm, weights_hbm, wg_hbm, wu_hbm, wd_hbm,
    out_ref,
    tok, gain, routes, weights, w_in, w_own, w_other,
    packed, gathered, rows_in, part_own, part_out, part_in, sums_out, sums_in, served, returned,
    small_sem, in_sem, own_sem, other_sem,
    z_send, z_recv, ag_send, ag_recv, d2d_send, d2d_recv, half_send, half_recv,
    rs_send, rs_recv, back_send, back_recv,
):
    z = lax.axis_index("ep")
    tp = lax.axis_index("tp")
    core = lax.rem(tp, 2)
    x = lax.div(tp, 2)
    tok_rows, width = tok.shape
    top = routes.shape[0]
    hidden_units = w_own.shape[0]
    offsets = ring_offsets(n_ep)
    all_rows = n_ep * cap
    rows = all_rows // CHUNKS
    half = rows // 2
    slots = n_ep // CHUNKS

    def chip(d):
        return lax.rem(x + d, CHIPS)

    def at_chip(d):
        return {"tp": chip(d) * 2 + core}

    def ring(offset):
        return lax.rem(z + offset + n_ep, n_ep)

    sibling = {"tp": x * 2 + 1 - core}

    def owner(p, d):
        return chip(d) * 2 + (core if p == 0 else 1 - core)

    barrier = pltpu.get_barrier_semaphore()
    for offset in offsets[:0:-1]:
        pl.semaphore_signal(barrier, inc=1, device_id={"ep": ring(offset)}, device_id_type=MESH)
    for d in (2, 6, 1, 7):
        pl.semaphore_signal(barrier, inc=1, device_id=at_chip(d), device_id_type=MESH)
    pl.semaphore_signal(barrier, inc=1, device_id=sibling, device_id_type=MESH)

    small = [
        pltpu.make_async_copy(source, target, small_sem.at[i])
        for i, (source, target) in enumerate(
            [(tok_hbm, tok), (routes_hbm, routes), (weights_hbm, weights), (gain_hbm, gain)]
        )
    ]
    for copy in small:
        copy.start()
    for p in range(2):
        for d in range(CHIPS):
            first = pl.multiple_of(owner(p, d) * width, width)
            k = p * CHIPS + d
            for j, source in enumerate((wg_hbm, wu_hbm)):
                pltpu.make_async_copy(
                    source.at[0, pl.ds(first, width), :],
                    w_in.at[pl.ds(k * width, width), pl.ds(j * hidden_units, hidden_units)],
                    in_sem,
                ).start()
    for p, target, sem in ((1, w_other, other_sem), (0, w_own, own_sem)):
        for d in range(CHIPS):
            first = pl.multiple_of(owner(p, d) * width, width)
            pltpu.make_async_copy(
                wd_hbm.at[0, :, pl.ds(first, width)], target.at[:, pl.ds(d * width, width)], sem
            ).start()

    small[0].wait()
    small[1].wait()
    place = lax.broadcasted_iota(jnp.int32, (all_rows, tok_rows), 0)
    place_expert = lax.div(place, cap)
    place_turn = lax.rem(place, cap)
    hits = [
        (jnp.broadcast_to(routes[k : k + 1, :], (all_rows, tok_rows)) == place_expert)
        for k in range(top)
    ]
    member = sum(hit.astype(jnp.float32) for hit in hits)
    earlier = (
        lax.broadcasted_iota(jnp.int32, (tok_rows, tok_rows), 0)
        < lax.broadcasted_iota(jnp.int32, (tok_rows, tok_rows), 1)
    ).astype(jnp.float32).astype(jnp.bfloat16)
    turn = jnp.dot(member.astype(jnp.bfloat16), earlier, preferred_element_type=jnp.float32)
    chosen = jnp.where(turn == place_turn.astype(jnp.float32), member, 0.0)
    outbox = jnp.dot(
        chosen.astype(jnp.bfloat16), tok[...], preferred_element_type=jnp.float32
    ).astype(jnp.bfloat16)
    packed[...] = outbox.reshape(n_ep, cap, width)

    pl.semaphore_wait(barrier, (n_ep - 1) + 4 + 1)

    sent = []

    def send(src, dst, send_sem, recv_sem, device):
        copy = pltpu.make_async_remote_copy(
            src_ref=src, dst_ref=dst, send_sem=send_sem, recv_sem=recv_sem,
            device_id=device, device_id_type=MESH,
        )
        copy.start()
        sent.append(copy)
        return copy

    def slot_rows(i):
        return pl.ds(i * cap, cap)

    dispatch = {}
    for i in range(n_ep - 1, 0, -1):
        expert = ring(-offsets[i])
        dispatch[i] = send(
            packed.at[expert], gathered.at[0, 0, slot_rows(i), :], z_send.at[i], z_recv.at[i],
            {"ep": expert},
        )
    gathered[0, 0, 0:cap, :] = packed[z]

    small[2].wait()
    mix = sum(
        jnp.where(hit, jnp.broadcast_to(weights[k : k + 1, :], (all_rows, tok_rows)), 0.0)
        for k, hit in enumerate(hits)
    ) * chosen
    mix_high = mix.astype(jnp.bfloat16)
    mix_low = (mix - mix_high.astype(jnp.float32)).astype(jnp.bfloat16)
    unit = (
        lax.broadcasted_iota(jnp.int32, (tok_rows, tok_rows), 0)
        == lax.broadcasted_iota(jnp.int32, (tok_rows, tok_rows), 1)
    ).astype(jnp.float32).astype(jnp.bfloat16)

    def flipped(value):
        return lax.dot_general(
            unit, value, (((1,), (1,)), ((), ())), preferred_element_type=jnp.float32
        ).astype(jnp.bfloat16)

    mix_high, mix_low = flipped(mix_high), flipped(mix_low)

    def span(c):
        return pl.ds(c * rows, rows)

    def top_half(c):
        return pl.ds(c * rows, half)

    def low_half(c):
        return pl.ds(c * rows + half, half)

    ag, d2d, halves, rs, back = {}, {}, {}, {}, {}

    def to_sibling(c, d, at, kind):
        d2d[c, kind] = send(
            gathered.at[0, d, at, :], gathered.at[1, d, at, :],
            d2d_send.at[c, kind], d2d_recv.at[c, kind], sibling,
        )

    def gather_own(c):
        for i in range(max(1, c * slots), (c + 1) * slots):
            dispatch[i].wait_recv()
        for kind, d, slot in ((2, 6, 2), (6, 2, 6), (1, 7, 1), (7, 1, 7)):
            ag[c, kind] = send(
                gathered.at[0, 0, span(c), :], gathered.at[0, slot, span(c), :],
                ag_send.at[c, kind], ag_recv.at[c, kind], at_chip(d),
            )
        to_sibling(c, 0, span(c), 0)

    def gather_relay(c):
        for slot, near, far, opposite, at, kind in (
            (2, 7, 6, 3, top_half(c), 4),
            (6, 1, 2, 5, low_half(c), 0),
        ):
            ag[c, slot].wait_recv()
            ag[c, kind] = send(
                gathered.at[0, slot, at, :], gathered.at[0, 4, at, :],
                ag_send.at[c, kind], ag_recv.at[c, kind], at_chip(far),
            )
            ag[c, opposite] = send(
                gathered.at[0, slot, span(c), :], gathered.at[0, opposite, span(c), :],
                ag_send.at[c, opposite], ag_recv.at[c, opposite], at_chip(near),
            )
            to_sibling(c, slot, span(c), slot)
        for slot in (1, 7):
            ag[c, slot].wait_recv()
            to_sibling(c, slot, span(c), slot)

    def gather_last(c):
        for slot in (3, 5):
            ag[c, slot].wait_recv()
            to_sibling(c, slot, span(c), slot)
        ag[c, 4].wait_recv()
        to_sibling(c, 4, top_half(c), 4)
        ag[c, 0].wait_recv()
        to_sibling(c, 4, low_half(c), 8)

    def feed(c):
        for kind in range(9):
            d2d[c, kind].wait_recv()
        blocks = [(p, d) for p in range(2) for d in range(CHIPS)]
        features = len(blocks) * width
        total = jnp.zeros((rows, width), jnp.float32)
        for p, d in blocks:
            total += gathered[p, d, span(c), :].astype(jnp.float32)
        average = jnp.sum(total, axis=1, keepdims=True) / features
        total = jnp.zeros((rows, width), jnp.float32)
        for p, d in blocks:
            off = gathered[p, d, span(c), :].astype(jnp.float32) - average
            total += off * off
        scale = lax.rsqrt(jnp.sum(total, axis=1, keepdims=True) / features + epsilon)
        for p, d in blocks:
            k = p * CHIPS + d
            off = gathered[p, d, span(c), :].astype(jnp.float32) - average
            rows_in[span(c), pl.ds(k * width, width)] = (
                off * scale * gain[pl.ds(owner(p, d), 1), :]
            ).astype(jnp.bfloat16)

    def expert(c):
        both = jnp.dot(rows_in[span(c), :], w_in[...], preferred_element_type=jnp.float32)
        gate_val, up_val = both[:, :hidden_units], both[:, hidden_units:]
        return (gate_val / (1.0 + jnp.exp(-gate_val)) * up_val).astype(jnp.bfloat16)

    def project(c, hidden):
        other = jnp.dot(hidden, w_other[...], preferred_element_type=jnp.float32)
        other = other.astype(jnp.bfloat16)
        for d in range(CHIPS):
            part_out[c, d] = other[:, d * width : (d + 1) * width]
        halves[c] = send(
            part_out.at[c], part_in.at[c], half_send.at[c], half_recv.at[c], sibling
        )
        part_own[c] = jnp.dot(hidden, w_own[...], preferred_element_type=jnp.float32)

    def chip_part(c, d):
        return part_own[c, :, pl.ds(d * width, width)] + part_in[c, d].astype(jnp.float32)

    def reduce_send(c, kind, d, source, slot, at=None):
        src, dst = sums_out.at[c, source], sums_in.at[c, slot]
        if at is not None:
            src, dst = src.at[at, :], dst.at[at, :]
        rs[c, kind] = send(src, dst, rs_send.at[c, kind], rs_recv.at[c, kind], at_chip(d))

    def reduce_first(c):
        halves[c].wait_recv()
        sums_out[c, 4] = chip_part(c, 4).astype(jnp.bfloat16)
        reduce_send(c, 4, 2, 4, 4, pl.ds(0, half))
        reduce_send(c, 0, 6, 4, 4, pl.ds(half, half))
        for d, near in ((3, 1), (5, 7), (1, 1), (7, 7)):
            sums_out[c, d] = chip_part(c, d).astype(jnp.bfloat16)
            reduce_send(c, d, near, d, d)

    def reduce_second(c):
        rs[c, 4].wait_recv()
        rs[c, 0].wait_recv()
        for d, near, at in ((2, 3, 0), (6, 5, half)):
            rs[c, near].wait_recv()
            value = chip_part(c, d) + sums_in[c, near].astype(jnp.float32)
            sums_out[c, d] = value.astype(jnp.bfloat16)
            sums_out[c, d, pl.ds(at, half), :] = (
                value[at : at + half] + sums_in[c, 4, pl.ds(at, half), :].astype(jnp.float32)
            ).astype(jnp.bfloat16)
            reduce_send(c, d, d, d, d)

    def finish(c):
        value = chip_part(c, 0)
        for slot in (1, 7, 2, 6):
            rs[c, slot].wait_recv()
            value += sums_in[c, slot].astype(jnp.float32)
        served[span(c), :] = value.astype(jnp.bfloat16)
        for i in range((c + 1) * slots - 1, max(1, c * slots) - 1, -1):
            back[i] = send(
                served.at[slot_rows(i), :], returned.at[z], back_send.at[i], back_recv.at[i],
                {"ep": ring(offsets[i])},
            )
        if c == 0:
            returned[z] = served[0:cap, :]

    gather_own(0)
    gather_own(1)
    gather_relay(0)
    gather_relay(1)
    gather_last(0)
    small[3].wait()
    feed(0)
    pltpu.make_async_copy(w_in, w_in, in_sem).wait()
    hidden = expert(0)
    pltpu.make_async_copy(w_other, w_other, other_sem).wait()
    pltpu.make_async_copy(w_own, w_own, own_sem).wait()
    project(0, hidden)
    gather_last(1)
    reduce_first(0)
    feed(1)
    project(1, expert(1))
    reduce_second(0)
    reduce_first(1)
    finish(0)
    reduce_second(1)
    finish(1)

    for i in range(n_ep - 1, 0, -1):
        back[i].wait_recv()
    values = returned[...].reshape(all_rows, width)
    out_ref[...] = (
        jnp.dot(mix_high, values, preferred_element_type=jnp.float32)
        + jnp.dot(mix_low, values, preferred_element_type=jnp.float32)
    ).astype(out_ref.dtype)
    for copy in sent:
        copy.wait_send()


def solution(mesh):
    n_ep, n_tp = mesh.shape["ep"], mesh.shape["tp"]

    def on_device(tokens, gain, routes, weights, w_gate, w_up, w_down):
        tok_rows, width = tokens.shape
        top = routes.shape[1]
        cap = min(tok_rows, 2 * tok_rows * top // n_ep)
        hidden_units = w_gate.shape[2]
        all_rows = n_ep * cap
        rows = all_rows // CHUNKS
        features = n_tp * width
        bf16, f32 = jnp.bfloat16, jnp.float32
        dma = pltpu.SemaphoreType.DMA
        return pl.pallas_call(
            functools.partial(kernel, n_ep, cap),
            out_shape=jax.ShapeDtypeStruct((tok_rows, width), bf16),
            in_specs=[pl.BlockSpec(memory_space=pltpu.HBM)] * 7,
            out_specs=pl.BlockSpec(memory_space=pltpu.VMEM),
            scratch_shapes=[
                pltpu.VMEM((tok_rows, width), bf16),
                pltpu.VMEM((n_tp, width), f32),
                pltpu.VMEM((top, tok_rows), jnp.int32),
                pltpu.VMEM((top, tok_rows), f32),
                pltpu.VMEM((features, 2 * hidden_units), bf16),
                pltpu.VMEM((hidden_units, features // 2), bf16),
                pltpu.VMEM((hidden_units, features // 2), bf16),
                pltpu.VMEM((n_ep, cap, width), bf16),
                pltpu.VMEM((2, CHIPS, all_rows, width), bf16),
                pltpu.VMEM((all_rows, features), bf16),
                pltpu.VMEM((CHUNKS, rows, features // 2), f32),
                pltpu.VMEM((CHUNKS, CHIPS, rows, width), bf16),
                pltpu.VMEM((CHUNKS, CHIPS, rows, width), bf16),
                pltpu.VMEM((CHUNKS, CHIPS, rows, width), bf16),
                pltpu.VMEM((CHUNKS, CHIPS, rows, width), bf16),
                pltpu.VMEM((all_rows, width), bf16),
                pltpu.VMEM((n_ep, cap, width), bf16),
                dma((4,)), dma, dma, dma,
                dma((n_ep,)), dma((n_ep,)),
                dma((CHUNKS, 8)), dma((CHUNKS, 8)),
                dma((CHUNKS, 9)), dma((CHUNKS, 9)),
                dma((CHUNKS,)), dma((CHUNKS,)),
                dma((CHUNKS, 8)), dma((CHUNKS, 8)),
                dma((n_ep,)), dma((n_ep,)),
            ],
            compiler_params=pltpu.CompilerParams(collective_id=0, has_side_effects=True),
        )(tokens, gain.reshape(n_tp, width), routes.T, weights.T, w_gate, w_up, w_down)

    in_specs = (
        P(("grp", "ep"), "tp"),
        P(),
        P(("grp", "ep"), None),
        P(("grp", "ep"), None),
        P("ep", None, "tp"),
        P("ep", None, "tp"),
        P("ep", "tp", None),
    )
    out_specs = P(("grp", "ep"), "tp")
    return jax.shard_map(
        on_device, mesh=mesh, in_specs=in_specs, out_specs=out_specs, check_vma=False
    )
```

```python
import functools

import jax
import jax.numpy as jnp
from jax import lax
from jax.experimental import pallas as pl
from jax.experimental.pallas import tpu as pltpu
from jax.sharding import PartitionSpec as P

MESH = pl.DeviceIdType.MESH
epsilon = 1e-05
SOURCES = 2


def kernel(
    n_ep, chips, cap,
    tok_hbm, gain_hbm, routes_hbm, weights_hbm, wg_hbm, wu_hbm, wd_hbm,
    out_ref,
    tok, gain, routes, weights, w_in, w_own, w_other,
    packed, gathered, part_own, part_out, part_in, sums_out, sums_in, served, returned,
    small_sem, in_sem, own_sem, other_sem, ready_z, ready_x, ready_core,
    z_send, z_recv, ag_send, ag_recv, d2d_send, d2d_recv, half_send, half_recv,
    rs_send, rs_recv, back_send, back_recv,
):
    z = lax.axis_index("ep")
    tp = lax.axis_index("tp")
    core = lax.rem(tp, 2)
    x = lax.div(tp, 2)
    tok_rows, width = tok.shape
    top = routes.shape[0]
    hidden_units = w_own.shape[0]
    all_rows = n_ep * cap
    chunks = n_ep // SOURCES
    rows = SOURCES * cap
    far_first = sorted(range(1, chips), key=lambda d: -min(d, chips - d))

    def chip(d):
        return lax.rem(x + d, chips)

    def at_chip(number):
        return {"tp": number * 2 + core}

    sibling = {"tp": x * 2 + 1 - core}

    def owner(p, d):
        return chip(d) * 2 + (core if p == 0 else 1 - core)

    def each(low, high, body):
        lax.fori_loop(low, high, lambda i, carry: (body(i), carry)[1], 0)

    barrier = pltpu.get_barrier_semaphore()

    def greet(device):
        pl.semaphore_signal(barrier, inc=1, device_id=device, device_id_type=MESH)

    each(z + 1, n_ep, lambda s: greet({"ep": s}))
    each(x + 1, chips, lambda s: greet(at_chip(s)))

    @pl.when(core == 0)
    def _():
        greet(sibling)

    small = [
        pltpu.make_async_copy(source, target, small_sem.at[i])
        for i, (source, target) in enumerate(
            [(tok_hbm, tok), (routes_hbm, routes), (weights_hbm, weights), (gain_hbm, gain)]
        )
    ]
    for copy in small:
        copy.start()
    for p in range(2):
        for d in range(chips):
            first = pl.multiple_of(owner(p, d) * width, width)
            k = p * chips + d
            for j, source in enumerate((wg_hbm, wu_hbm)):
                pltpu.make_async_copy(
                    source.at[0, pl.ds(first, width), :],
                    w_in.at[pl.ds(k * width, width), pl.ds(j * hidden_units, hidden_units)],
                    in_sem,
                ).start()
    for p, target, sem in ((1, w_other, other_sem), (0, w_own, own_sem)):
        for d in range(chips):
            first = pl.multiple_of(owner(p, d) * width, width)
            pltpu.make_async_copy(
                wd_hbm.at[0, :, pl.ds(first, width)], target.at[:, pl.ds(d * width, width)], sem
            ).start()

    below = z + x + core

    @pl.when(below > 0)
    def _():
        pl.semaphore_wait(barrier, below)

    def answer(semaphore, device):
        pl.semaphore_signal(semaphore, inc=1, device_id=device, device_id_type=MESH)

    each(0, z, lambda s: answer(ready_z.at[z], {"ep": s}))
    each(0, x, lambda s: answer(ready_x.at[x], at_chip(s)))

    @pl.when(core == 1)
    def _():
        answer(ready_core, sibling)

    small[0].wait()
    small[1].wait()
    place = lax.broadcasted_iota(jnp.int32, (all_rows, tok_rows), 0)
    place_expert = lax.div(place, cap)
    place_turn = lax.rem(place, cap)
    hits = [
        (jnp.broadcast_to(routes[k : k + 1, :], (all_rows, tok_rows)) == place_expert)
        for k in range(top)
    ]
    member = sum(hit.astype(jnp.float32) for hit in hits)
    earlier = (
        lax.broadcasted_iota(jnp.int32, (tok_rows, tok_rows), 0)
        < lax.broadcasted_iota(jnp.int32, (tok_rows, tok_rows), 1)
    ).astype(jnp.float32).astype(jnp.bfloat16)
    turn = jnp.dot(member.astype(jnp.bfloat16), earlier, preferred_element_type=jnp.float32)
    chosen = jnp.where(turn == place_turn.astype(jnp.float32), member, 0.0)
    outbox = jnp.dot(
        chosen.astype(jnp.bfloat16), tok[...], preferred_element_type=jnp.float32
    ).astype(jnp.bfloat16)
    packed[...] = outbox.reshape(n_ep, cap, width)

    def remote(src, dst, send_sem, recv_sem, device):
        return pltpu.make_async_remote_copy(
            src_ref=src, dst_ref=dst, send_sem=send_sem, recv_sem=recv_sem,
            device_id=device, device_id_type=MESH,
        )

    def landed(ref, semaphore):
        pltpu.make_async_copy(ref, ref, semaphore).wait()

    def dispatch(s):
        remote(
            packed.at[s], gathered.at[0, 0, z], z_send.at[s], z_recv.at[z], {"ep": s}
        ).start()

    each(0, z, dispatch)
    gathered[0, 0, z] = packed[z]

    small[2].wait()
    mix = sum(
        jnp.where(hit, jnp.broadcast_to(weights[k : k + 1, :], (all_rows, tok_rows)), 0.0)
        for k, hit in enumerate(hits)
    ) * chosen
    mix_high = mix.astype(jnp.bfloat16)
    mix_low = (mix - mix_high.astype(jnp.float32)).astype(jnp.bfloat16)
    unit = (
        lax.broadcasted_iota(jnp.int32, (tok_rows, tok_rows), 0)
        == lax.broadcasted_iota(jnp.int32, (tok_rows, tok_rows), 1)
    ).astype(jnp.float32).astype(jnp.bfloat16)

    def flipped(value):
        return lax.dot_general(
            unit, value, (((1,), (1,)), ((), ())), preferred_element_type=jnp.float32
        ).astype(jnp.bfloat16)

    mix_high, mix_low = flipped(mix_high), flipped(mix_low)

    def span(c):
        return pl.ds(c * SOURCES, SOURCES)

    def dispatch_up(c):
        for j in range(SOURCES):
            s = c * SOURCES + j

            @pl.when(s > z)
            def _():
                pl.semaphore_wait(ready_z.at[s], 1)
                dispatch(s)

    def gather(c):
        for j in range(SOURCES):
            s = c * SOURCES + j

            @pl.when(s != z)
            def _():
                landed(gathered.at[0, 0, s], z_recv.at[s])

        for d in far_first:
            remote(
                gathered.at[0, 0, span(c)], gathered.at[0, chips - d, span(c)],
                ag_send.at[c], ag_recv.at[c], at_chip(chip(d)),
            ).start()

    def across(c):
        return remote(
            gathered.at[0, :, span(c)], gathered.at[1, :, span(c)],
            d2d_send.at[c], d2d_recv.at[c], sibling,
        )

    def share(c):
        landed(gathered.at[0, 1:, span(c)], ag_recv.at[c])
        across(c).start()

    def half(c):
        return remote(
            part_out.at[c], part_in.at[c], half_send.at[c], half_recv.at[c], sibling
        )

    def serve(c):
        across(c).wait_recv()
        blocks = [(p, d) for p in range(2) for d in range(chips)]
        features = len(blocks) * width
        values = [
            gathered[p, d, span(c)].reshape(rows, width).astype(jnp.float32) for p, d in blocks
        ]
        average = jnp.sum(sum(values), axis=1, keepdims=True) / features
        values = [value - average for value in values]
        spread = jnp.sum(sum(v * v for v in values), axis=1, keepdims=True) / features
        scale = lax.rsqrt(spread + epsilon)
        normed = [
            (value * scale * gain[pl.ds(owner(p, d), 1), :]).astype(jnp.bfloat16)
            for value, (p, d) in zip(values, blocks)
        ]
        both = jnp.dot(
            jnp.concatenate(normed, axis=1), w_in[...], preferred_element_type=jnp.float32
        )
        gate_val, up_val = both[:, :hidden_units], both[:, hidden_units:]
        hidden = (gate_val / (1.0 + jnp.exp(-gate_val)) * up_val).astype(jnp.bfloat16)
        other = jnp.dot(hidden, w_other[...], preferred_element_type=jnp.float32)
        other = other.astype(jnp.bfloat16)
        for d in range(chips):
            part_out[c, d] = other[:, d * width : (d + 1) * width]
        half(c).start()
        own = jnp.dot(hidden, w_own[...], preferred_element_type=jnp.float32)
        for d in range(chips):
            part_own[c, d] = own[:, d * width : (d + 1) * width]

    def reduce(c):
        half(c).wait_recv()
        for d in far_first:
            sums_out[c, d] = (part_own[c, d] + part_in[c, d].astype(jnp.float32)).astype(
                jnp.bfloat16
            )
            remote(
                sums_out.at[c, d], sums_in.at[c, chips - d], rs_send.at[c], rs_recv.at[c],
                at_chip(chip(d)),
            ).start()

    def back(s):
        return remote(
            served.at[s], returned.at[z], back_send.at[s], back_recv.at[z], {"ep": s}
        )

    def finish(c):
        landed(sums_in.at[c, 1:], rs_recv.at[c])
        value = part_own[c, 0] + part_in[c, 0].astype(jnp.float32)
        for d in range(1, chips):
            value += sums_in[c, d].astype(jnp.float32)
        served[span(c)] = value.astype(jnp.bfloat16).reshape(SOURCES, cap, width)
        for j in range(SOURCES):
            s = c * SOURCES + j

            @pl.when(s != z)
            def _():
                back(s).start()

            @pl.when(s == z)
            def _():
                returned[z] = served[z]

    small[3].wait()
    landed(w_in, in_sem)
    landed(w_other, other_sem)
    landed(w_own, own_sem)
    each(x + 1, chips, lambda s: pl.semaphore_wait(ready_x.at[s], 1))

    @pl.when(core == 0)
    def _():
        pl.semaphore_wait(ready_core, 1)

    dispatch_up(0)

    def step(i):
        pl.when(i + 1 < chunks)(lambda: dispatch_up(i + 1))
        pl.when(i < chunks)(lambda: gather(i))
        pl.when((i >= 2) & (i < chunks + 2))(lambda: reduce(i - 2))

        @pl.when((i >= 1) & (i < chunks + 1))
        def _():
            share(i - 1)
            serve(i - 1)

        pl.when(i >= 3)(lambda: finish(i - 3))

    each(0, chunks + 3, step)

    def others(body):
        each(0, z, body)
        each(z + 1, n_ep, body)

    others(lambda e: landed(returned.at[e], back_recv.at[e]))
    values = returned[...].reshape(all_rows, width)
    out_ref[...] = (
        jnp.dot(mix_high, values, preferred_element_type=jnp.float32)
        + jnp.dot(mix_low, values, preferred_element_type=jnp.float32)
    ).astype(out_ref.dtype)

    def settle(s):
        landed(packed.at[s], z_send.at[s])
        landed(served.at[s], back_send.at[s])

    others(settle)

    def settle_chunk(c):
        landed(gathered.at[0, 1:, span(c)], ag_send.at[c])
        across(c).wait_send()
        half(c).wait_send()
        landed(sums_out.at[c, 1:], rs_send.at[c])

    each(0, chunks, settle_chunk)


def solution(mesh):
    n_ep, n_tp = mesh.shape["ep"], mesh.shape["tp"]
    chips = n_tp // 2
    chunks = n_ep // SOURCES

    def on_device(tokens, gain, routes, weights, w_gate, w_up, w_down):
        tok_rows, width = tokens.shape
        top = routes.shape[1]
        cap = min(tok_rows, 2 * tok_rows * top // n_ep)
        hidden_units = w_gate.shape[2]
        rows = SOURCES * cap
        features = n_tp * width
        bf16, f32 = jnp.bfloat16, jnp.float32
        dma = pltpu.SemaphoreType.DMA
        regular = pltpu.SemaphoreType.REGULAR
        return pl.pallas_call(
            functools.partial(kernel, n_ep, chips, cap),
            out_shape=jax.ShapeDtypeStruct((tok_rows, width), bf16),
            in_specs=[pl.BlockSpec(memory_space=pltpu.HBM)] * 7,
            out_specs=pl.BlockSpec(memory_space=pltpu.VMEM),
            scratch_shapes=[
                pltpu.VMEM((tok_rows, width), bf16),
                pltpu.VMEM((n_tp, width), f32),
                pltpu.VMEM((top, tok_rows), jnp.int32),
                pltpu.VMEM((top, tok_rows), f32),
                pltpu.VMEM((features, 2 * hidden_units), bf16),
                pltpu.VMEM((hidden_units, features // 2), bf16),
                pltpu.VMEM((hidden_units, features // 2), bf16),
                pltpu.VMEM((n_ep, cap, width), bf16),
                pltpu.VMEM((2, chips, n_ep, cap, width), bf16),
                pltpu.VMEM((chunks, chips, rows, width), f32),
                pltpu.VMEM((chunks, chips, rows, width), bf16),
                pltpu.VMEM((chunks, chips, rows, width), bf16),
                pltpu.VMEM((chunks, chips, rows, width), bf16),
                pltpu.VMEM((chunks, chips, rows, width), bf16),
                pltpu.VMEM((n_ep, cap, width), bf16),
                pltpu.VMEM((n_ep, cap, width), bf16),
                dma((4,)), dma, dma, dma,
                regular((n_ep,)), regular((chips,)), regular,
                dma((n_ep,)), dma((n_ep,)),
                dma((chunks,)), dma((chunks,)),
                dma((chunks,)), dma((chunks,)),
                dma((chunks,)), dma((chunks,)),
                dma((chunks,)), dma((chunks,)),
                dma((n_ep,)), dma((n_ep,)),
            ],
            compiler_params=pltpu.CompilerParams(collective_id=0, has_side_effects=True),
        )(tokens, gain.reshape(n_tp, width), routes.T, weights.T, w_gate, w_up, w_down)

    in_specs = (
        P(("grp", "ep"), "tp"),
        P(),
        P(("grp", "ep"), None),
        P(("grp", "ep"), None),
        P("ep", None, "tp"),
        P("ep", None, "tp"),
        P("ep", "tp", None),
    )
    out_specs = P(("grp", "ep"), "tp")
    return jax.shard_map(
        on_device, mesh=mesh, in_specs=in_specs, out_specs=out_specs, check_vma=False
    )
```

```python
import functools

import jax
import jax.numpy as jnp
from jax import lax
from jax.experimental import pallas as pl
from jax.experimental.pallas import tpu as pltpu
from jax.sharding import PartitionSpec as P

MESH = pl.DeviceIdType.MESH
epsilon = 1e-05
CHIPS = 8
CUTS = (0, 2, 8, 16)
CHUNKS = len(CUTS) - 1
DIRECT = (0,)


def kernel(
    n_ep, cap,
    tok_hbm, gain_hbm, routes_hbm, weights_hbm, wg_hbm, wu_hbm, wd_hbm,
    out_ref,
    tok, gain, routes, weights, w_in, w_own, w_other,
    packed, gathered, rows_in, part_own, part_out, part_in, sums_out, sums_in, served, returned,
    small_sem, in_sem, own_sem, other_sem,
    z_send, z_recv, ag_send, ag_recv, d2d_send, d2d_recv, half_send, half_recv,
    rs_send, rs_recv, back_send, back_recv,
):
    z = lax.axis_index("ep")
    tp = lax.axis_index("tp")
    core = lax.rem(tp, 2)
    x = lax.div(tp, 2)
    tok_rows, width = tok.shape
    top = routes.shape[0]
    hidden_units = w_own.shape[0]
    all_rows = n_ep * cap
    cuts = [cut * n_ep // CUTS[-1] for cut in CUTS]
    firsts = [cut * cap for cut in cuts]
    far_first = sorted(range(1, CHIPS), key=lambda d: -min(d, CHIPS - d))

    def chip(d):
        return lax.rem(x + d, CHIPS)

    def at_chip(d):
        return {"tp": chip(d) * 2 + core}

    def ring(offset):
        return lax.rem(z + offset + n_ep, n_ep)

    sibling = {"tp": x * 2 + 1 - core}

    def owner(p, d):
        return chip(d) * 2 + (core if p == 0 else 1 - core)

    barrier = pltpu.get_barrier_semaphore()
    for offset in range(1, n_ep):
        pl.semaphore_signal(barrier, inc=1, device_id={"ep": ring(offset)}, device_id_type=MESH)
    for d in far_first:
        pl.semaphore_signal(barrier, inc=1, device_id=at_chip(d), device_id_type=MESH)
    pl.semaphore_signal(barrier, inc=1, device_id=sibling, device_id_type=MESH)

    small = [
        pltpu.make_async_copy(source, target, small_sem.at[i])
        for i, (source, target) in enumerate(
            [(tok_hbm, tok), (routes_hbm, routes), (weights_hbm, weights), (gain_hbm, gain)]
        )
    ]
    for copy in small:
        copy.start()
    for p in range(2):
        for d in range(CHIPS):
            first = pl.multiple_of(owner(p, d) * width, width)
            k = p * CHIPS + d
            for j, source in enumerate((wg_hbm, wu_hbm)):
                pltpu.make_async_copy(
                    source.at[0, pl.ds(first, width), :],
                    w_in.at[pl.ds(k * width, width), pl.ds(j * hidden_units, hidden_units)],
                    in_sem,
                ).start()
    for p, target, sem in ((1, w_other, other_sem), (0, w_own, own_sem)):
        for d in range(CHIPS):
            first = pl.multiple_of(owner(p, d) * width, width)
            pltpu.make_async_copy(
                wd_hbm.at[0, :, pl.ds(first, width)], target.at[:, pl.ds(d * width, width)], sem
            ).start()

    small[0].wait()
    small[1].wait()
    place = lax.broadcasted_iota(jnp.int32, (all_rows, tok_rows), 0)
    place_expert = lax.div(place, cap)
    place_turn = lax.rem(place, cap)
    hits = [
        (jnp.broadcast_to(routes[k : k + 1, :], (all_rows, tok_rows)) == place_expert)
        for k in range(top)
    ]
    member = sum(hit.astype(jnp.float32) for hit in hits)
    earlier = (
        lax.broadcasted_iota(jnp.int32, (tok_rows, tok_rows), 0)
        < lax.broadcasted_iota(jnp.int32, (tok_rows, tok_rows), 1)
    ).astype(jnp.float32).astype(jnp.bfloat16)
    turn = jnp.dot(member.astype(jnp.bfloat16), earlier, preferred_element_type=jnp.float32)
    chosen = jnp.where(turn == place_turn.astype(jnp.float32), member, 0.0)
    outbox = jnp.dot(
        chosen.astype(jnp.bfloat16), tok[...], preferred_element_type=jnp.float32
    ).astype(jnp.bfloat16)
    packed[...] = outbox.reshape(n_ep, cap, width)

    pl.semaphore_wait(barrier, (n_ep - 1) + (CHIPS - 1) + 1)

    sent = []

    def send(src, dst, send_sem, recv_sem, device):
        copy = pltpu.make_async_remote_copy(
            src_ref=src, dst_ref=dst, send_sem=send_sem, recv_sem=recv_sem,
            device_id=device, device_id_type=MESH,
        )
        copy.start()
        sent.append(copy)
        return copy

    def landed(ref, semaphore):
        pltpu.make_async_copy(ref, ref, semaphore).wait()

    def slot_rows(i):
        return pl.ds(pl.multiple_of(i * cap, cap), cap)

    for offset in sorted(range(1, n_ep), key=lambda o: -min(o, n_ep - o)):
        expert = ring(offset)
        send(
            packed.at[expert], gathered.at[0, 0, slot_rows(z), :], z_send.at[offset], z_recv.at[z],
            {"ep": expert},
        )
    gathered[0, 0, slot_rows(z), :] = packed[z]

    small[2].wait()
    mix = sum(
        jnp.where(hit, jnp.broadcast_to(weights[k : k + 1, :], (all_rows, tok_rows)), 0.0)
        for k, hit in enumerate(hits)
    ) * chosen
    mix_high = mix.astype(jnp.bfloat16)
    mix_low = (mix - mix_high.astype(jnp.float32)).astype(jnp.bfloat16)
    unit = (
        lax.broadcasted_iota(jnp.int32, (tok_rows, tok_rows), 0)
        == lax.broadcasted_iota(jnp.int32, (tok_rows, tok_rows), 1)
    ).astype(jnp.float32).astype(jnp.bfloat16)

    def flipped(value):
        return lax.dot_general(
            unit, value, (((1,), (1,)), ((), ())), preferred_element_type=jnp.float32
        ).astype(jnp.bfloat16)

    mix_high, mix_low = flipped(mix_high), flipped(mix_low)

    def span(c):
        return pl.ds(firsts[c], firsts[c + 1] - firsts[c])

    def halved(c):
        return (firsts[c + 1] - firsts[c]) // 2

    def top_half(c):
        return pl.ds(firsts[c], halved(c))

    def low_half(c):
        return pl.ds(firsts[c] + halved(c), halved(c))

    ag, d2d, halves, rs = {}, {}, {}, {}

    def to_sibling(c, d, at, kind):
        d2d[c, kind] = send(
            gathered.at[0, d, at, :], gathered.at[1, d, at, :],
            d2d_send.at[c, kind], d2d_recv.at[c, kind], sibling,
        )

    def gather_own(c):
        for s in range(cuts[c], cuts[c + 1]):

            @pl.when(s != z)
            def _():
                landed(gathered.at[0, 0, slot_rows(s), :], z_recv.at[s])

        if c in DIRECT:
            hops = [(CHIPS - d, d) for d in far_first]
        else:
            hops = [(2, 6), (6, 2), (1, 7), (7, 1)]
        for slot, d in hops:
            ag[c, slot] = send(
                gathered.at[0, 0, span(c), :], gathered.at[0, slot, span(c), :],
                ag_send.at[c, slot], ag_recv.at[c, slot], at_chip(d),
            )
        to_sibling(c, 0, span(c), 0)

    def share(c):
        for slot in (1, 7, 2, 6, 3, 5, 4):
            ag[c, slot].wait_recv()
            to_sibling(c, slot, span(c), slot)

    def gather_relay(c):
        for slot, near, far, opposite, at, kind in (
            (2, 7, 6, 3, top_half(c), 4),
            (6, 1, 2, 5, low_half(c), 0),
        ):
            ag[c, slot].wait_recv()
            ag[c, kind] = send(
                gathered.at[0, slot, at, :], gathered.at[0, 4, at, :],
                ag_send.at[c, kind], ag_recv.at[c, kind], at_chip(far),
            )
            ag[c, opposite] = send(
                gathered.at[0, slot, span(c), :], gathered.at[0, opposite, span(c), :],
                ag_send.at[c, opposite], ag_recv.at[c, opposite], at_chip(near),
            )
            to_sibling(c, slot, span(c), slot)
        for slot in (1, 7):
            ag[c, slot].wait_recv()
            to_sibling(c, slot, span(c), slot)

    def gather_last(c):
        for slot in (3, 5):
            ag[c, slot].wait_recv()
            to_sibling(c, slot, span(c), slot)
        ag[c, 4].wait_recv()
        to_sibling(c, 4, top_half(c), 4)
        ag[c, 0].wait_recv()
        to_sibling(c, 4, low_half(c), 8)

    def feed(c):
        for kind in range(8 if c in DIRECT else 9):
            d2d[c, kind].wait_recv()
        blocks = [(p, d) for p in range(2) for d in range(CHIPS)]
        features = len(blocks) * width
        shape = (firsts[c + 1] - firsts[c], width)
        total = jnp.zeros(shape, jnp.float32)
        for p, d in blocks:
            total += gathered[p, d, span(c), :].astype(jnp.float32)
        average = jnp.sum(total, axis=1, keepdims=True) / features
        total = jnp.zeros(shape, jnp.float32)
        for p, d in blocks:
            off = gathered[p, d, span(c), :].astype(jnp.float32) - average
            total += off * off
        scale = lax.rsqrt(jnp.sum(total, axis=1, keepdims=True) / features + epsilon)
        for p, d in blocks:
            k = p * CHIPS + d
            off = gathered[p, d, span(c), :].astype(jnp.float32) - average
            rows_in[span(c), pl.ds(k * width, width)] = (
                off * scale * gain[pl.ds(owner(p, d), 1), :]
            ).astype(jnp.bfloat16)

    def expert(c):
        both = jnp.dot(rows_in[span(c), :], w_in[...], preferred_element_type=jnp.float32)
        gate_val, up_val = both[:, :hidden_units], both[:, hidden_units:]
        return (gate_val / (1.0 + jnp.exp(-gate_val)) * up_val).astype(jnp.bfloat16)

    def project(c, hidden):
        other = jnp.dot(hidden, w_other[...], preferred_element_type=jnp.float32)
        other = other.astype(jnp.bfloat16)
        for d in range(CHIPS):
            part_out[d, span(c), :] = other[:, d * width : (d + 1) * width]
        halves[c] = send(
            part_out.at[:, span(c), :], part_in.at[:, span(c), :],
            half_send.at[c], half_recv.at[c], sibling,
        )
        own = jnp.dot(hidden, w_own[...], preferred_element_type=jnp.float32)
        for d in range(CHIPS):
            part_own[d, span(c), :] = own[:, d * width : (d + 1) * width]

    def serve(c):
        feed(c)
        project(c, expert(c))

    def chip_part(d, at):
        return part_own[d, at, :] + part_in[d, at, :].astype(jnp.float32)

    def reduce_send(c, kind, d, source, slot, at):
        rs[c, kind] = send(
            sums_out.at[source, at, :], sums_in.at[slot, at, :],
            rs_send.at[c, kind], rs_recv.at[c, kind], at_chip(d),
        )

    def reduce_direct(c):
        halves[c].wait_recv()
        for d in far_first:
            sums_out[d, span(c), :] = chip_part(d, span(c)).astype(jnp.bfloat16)
            reduce_send(c, CHIPS - d, d, d, CHIPS - d, span(c))

    def finish_direct(c):
        value = chip_part(0, span(c))
        for slot in far_first:
            rs[c, slot].wait_recv()
            value += sums_in[slot, span(c), :].astype(jnp.float32)
        give_back(c, value)

    def reduce_first(c):
        halves[c].wait_recv()
        sums_out[4, span(c), :] = chip_part(4, span(c)).astype(jnp.bfloat16)
        reduce_send(c, 4, 2, 4, 4, top_half(c))
        reduce_send(c, 0, 6, 4, 4, low_half(c))
        for d, near in ((3, 1), (5, 7), (1, 1), (7, 7)):
            sums_out[d, span(c), :] = chip_part(d, span(c)).astype(jnp.bfloat16)
            reduce_send(c, d, near, d, d, span(c))

    def reduce_second(c):
        rs[c, 4].wait_recv()
        rs[c, 0].wait_recv()
        for d, near, joined, alone in (
            (2, 3, top_half(c), low_half(c)), (6, 5, low_half(c), top_half(c))
        ):
            rs[c, near].wait_recv()
            sums_out[d, joined, :] = (
                chip_part(d, joined)
                + sums_in[near, joined, :].astype(jnp.float32)
                + sums_in[4, joined, :].astype(jnp.float32)
            ).astype(jnp.bfloat16)
            sums_out[d, alone, :] = (
                chip_part(d, alone) + sums_in[near, alone, :].astype(jnp.float32)
            ).astype(jnp.bfloat16)
            reduce_send(c, d, d, d, d, span(c))

    def finish(c):
        value = chip_part(0, span(c))
        for slot in (1, 7, 2, 6):
            rs[c, slot].wait_recv()
            value += sums_in[slot, span(c), :].astype(jnp.float32)
        give_back(c, value)

    def back(s):
        return pltpu.make_async_remote_copy(
            src_ref=served.at[slot_rows(s), :], dst_ref=returned.at[z],
            send_sem=back_send.at[s], recv_sem=back_recv.at[z],
            device_id={"ep": s}, device_id_type=MESH,
        )

    def give_back(c, value):
        served[span(c), :] = value.astype(jnp.bfloat16)
        for s in range(cuts[c], cuts[c + 1]):

            @pl.when(s != z)
            def _():
                back(s).start()

            @pl.when(s == z)
            def _():
                returned[z] = served[slot_rows(s), :]

    gather_own(0)
    gather_own(1)
    gather_own(2)
    small[3].wait()
    pltpu.make_async_copy(w_in, w_in, in_sem).wait()
    pltpu.make_async_copy(w_other, w_other, other_sem).wait()
    pltpu.make_async_copy(w_own, w_own, own_sem).wait()
    share(0)
    gather_relay(1)
    serve(0)
    gather_relay(2)
    gather_last(1)
    reduce_direct(0)
    serve(1)
    gather_last(2)
    reduce_first(1)
    serve(2)
    finish_direct(0)
    reduce_second(1)
    reduce_first(2)
    finish(1)
    reduce_second(2)
    finish(2)

    for e in range(n_ep):

        @pl.when(e != z)
        def _():
            landed(returned.at[e], back_recv.at[e])

    values = returned[...].reshape(all_rows, width)
    out_ref[...] = (
        jnp.dot(mix_high, values, preferred_element_type=jnp.float32)
        + jnp.dot(mix_low, values, preferred_element_type=jnp.float32)
    ).astype(out_ref.dtype)
    for copy in sent:
        copy.wait_send()
    for s in range(n_ep):

        @pl.when(s != z)
        def _():
            back(s).wait_send()


def solution(mesh):
    n_ep, n_tp = mesh.shape["ep"], mesh.shape["tp"]

    def on_device(tokens, gain, routes, weights, w_gate, w_up, w_down):
        tok_rows, width = tokens.shape
        top = routes.shape[1]
        cap = min(tok_rows, 2 * tok_rows * top // n_ep)
        hidden_units = w_gate.shape[2]
        all_rows = n_ep * cap
        features = n_tp * width
        bf16, f32 = jnp.bfloat16, jnp.float32
        dma = pltpu.SemaphoreType.DMA
        return pl.pallas_call(
            functools.partial(kernel, n_ep, cap),
            out_shape=jax.ShapeDtypeStruct((tok_rows, width), bf16),
            in_specs=[pl.BlockSpec(memory_space=pltpu.HBM)] * 7,
            out_specs=pl.BlockSpec(memory_space=pltpu.VMEM),
            scratch_shapes=[
                pltpu.VMEM((tok_rows, width), bf16),
                pltpu.VMEM((n_tp, width), f32),
                pltpu.VMEM((top, tok_rows), jnp.int32),
                pltpu.VMEM((top, tok_rows), f32),
                pltpu.VMEM((features, 2 * hidden_units), bf16),
                pltpu.VMEM((hidden_units, features // 2), bf16),
                pltpu.VMEM((hidden_units, features // 2), bf16),
                pltpu.VMEM((n_ep, cap, width), bf16),
                pltpu.VMEM((2, CHIPS, all_rows, width), bf16),
                pltpu.VMEM((all_rows, features), bf16),
                pltpu.VMEM((CHIPS, all_rows, width), f32),
                pltpu.VMEM((CHIPS, all_rows, width), bf16),
                pltpu.VMEM((CHIPS, all_rows, width), bf16),
                pltpu.VMEM((CHIPS, all_rows, width), bf16),
                pltpu.VMEM((CHIPS, all_rows, width), bf16),
                pltpu.VMEM((all_rows, width), bf16),
                pltpu.VMEM((n_ep, cap, width), bf16),
                dma((4,)), dma, dma, dma,
                dma((n_ep,)), dma((n_ep,)),
                dma((CHUNKS, 8)), dma((CHUNKS, 8)),
                dma((CHUNKS, 9)), dma((CHUNKS, 9)),
                dma((CHUNKS,)), dma((CHUNKS,)),
                dma((CHUNKS, 8)), dma((CHUNKS, 8)),
                dma((n_ep,)), dma((n_ep,)),
            ],
            compiler_params=pltpu.CompilerParams(collective_id=0, has_side_effects=True),
        )(tokens, gain.reshape(n_tp, width), routes.T, weights.T, w_gate, w_up, w_down)

    in_specs = (
        P(("grp", "ep"), "tp"),
        P(),
        P(("grp", "ep"), None),
        P(("grp", "ep"), None),
        P("ep", None, "tp"),
        P("ep", None, "tp"),
        P("ep", "tp", None),
    )
    out_specs = P(("grp", "ep"), "tp")
    return jax.shard_map(
        on_device, mesh=mesh, in_specs=in_specs, out_specs=out_specs, check_vma=False
    )
```

```python
import functools

import jax
import jax.numpy as jnp
from jax import lax
from jax.experimental import pallas as pl
from jax.experimental.pallas import tpu as pltpu
from jax.sharding import PartitionSpec as P

MESH = pl.DeviceIdType.MESH
epsilon = 1e-05
CHIPS = 8
ORDER = (0, 1, 2, 3, 4, 11, 12, 13, 5, 6, 9, 10, 7, 8, 14, 15)
CUTS = (0, 2, 8, 12, 16)
CHUNKS = len(CUTS) - 1
DIRECT = (0,)
LATE = 2


def kernel(
    n_ep, cap,
    tok_hbm, gain_hbm, routes_hbm, weights_hbm, wg_hbm, wu_hbm, wd_hbm,
    out_ref,
    tok, gain, routes, weights, w_in, w_own, w_other,
    packed, gathered, rows_in, part_own, part_out, part_in, sums_out, sums_in, served, returned,
    small_sem, in_sem, own_sem, other_sem, ready,
    z_send, z_recv, ag_send, ag_recv, d2d_send, d2d_recv, half_send, half_recv,
    rs_send, rs_recv, back_send, back_recv,
):
    z = lax.axis_index("ep")
    tp = lax.axis_index("tp")
    core = lax.rem(tp, 2)
    x = lax.div(tp, 2)
    tok_rows, width = tok.shape
    top = routes.shape[0]
    hidden_units = w_own.shape[0]
    all_rows = n_ep * cap
    firsts = [cut * cap for cut in CUTS]
    early_count = n_ep - LATE
    far_first = sorted(range(1, CHIPS), key=lambda d: -min(d, CHIPS - d))

    def chip(d):
        return lax.rem(x + d, CHIPS)

    def at_chip(d):
        return {"tp": chip(d) * 2 + core}

    sibling = {"tp": x * 2 + 1 - core}

    def owner(p, d):
        return chip(d) * 2 + (core if p == 0 else 1 - core)

    barrier = pltpu.get_barrier_semaphore()

    def greet(device):
        pl.semaphore_signal(barrier, inc=1, device_id=device, device_id_type=MESH)

    for s in range(n_ep - 1, -1, -1):

        @pl.when((s != z) & ((z < early_count) if s < early_count else (z >= 0)))
        def _():
            greet({"ep": s})

    for d in far_first:
        greet(at_chip(d))
    greet(sibling)

    small = [
        pltpu.make_async_copy(source, target, small_sem.at[i])
        for i, (source, target) in enumerate(
            [(tok_hbm, tok), (routes_hbm, routes), (weights_hbm, weights), (gain_hbm, gain)]
        )
    ]
    for copy in small:
        copy.start()
    for p in range(2):
        for d in range(CHIPS):
            first = pl.multiple_of(owner(p, d) * width, width)
            k = p * CHIPS + d
            for j, source in enumerate((wg_hbm, wu_hbm)):
                pltpu.make_async_copy(
                    source.at[0, pl.ds(first, width), :],
                    w_in.at[pl.ds(k * width, width), pl.ds(j * hidden_units, hidden_units)],
                    in_sem,
                ).start()
    for p, target, sem in ((1, w_other, other_sem), (0, w_own, own_sem)):
        for d in range(CHIPS):
            first = pl.multiple_of(owner(p, d) * width, width)
            pltpu.make_async_copy(
                wd_hbm.at[0, :, pl.ds(first, width)], target.at[:, pl.ds(d * width, width)], sem
            ).start()

    small[0].wait()
    small[1].wait()
    place = lax.broadcasted_iota(jnp.int32, (all_rows, tok_rows), 0)
    place_expert = lax.div(place, cap)
    place_turn = lax.rem(place, cap)
    hits = [
        (jnp.broadcast_to(routes[k : k + 1, :], (all_rows, tok_rows)) == place_expert)
        for k in range(top)
    ]
    member = sum(hit.astype(jnp.float32) for hit in hits)
    earlier = (
        lax.broadcasted_iota(jnp.int32, (tok_rows, tok_rows), 0)
        < lax.broadcasted_iota(jnp.int32, (tok_rows, tok_rows), 1)
    ).astype(jnp.float32).astype(jnp.bfloat16)
    turn = jnp.dot(member.astype(jnp.bfloat16), earlier, preferred_element_type=jnp.float32)
    chosen = jnp.where(turn == place_turn.astype(jnp.float32), member, 0.0)
    outbox = jnp.dot(
        chosen.astype(jnp.bfloat16), tok[...], preferred_element_type=jnp.float32
    ).astype(jnp.bfloat16)
    packed[...] = outbox.reshape(n_ep, cap, width)

    @pl.when(z < early_count)
    def _():
        pl.semaphore_wait(barrier, early_count - 1 + CHIPS)

    @pl.when(z >= early_count)
    def _():
        pl.semaphore_wait(barrier, n_ep - 1 + CHIPS)
        for s in range(early_count):
            pl.semaphore_signal(
                ready.at[z - early_count], inc=1, device_id={"ep": s}, device_id_type=MESH
            )

    def send(src, dst, send_sem, recv_sem, device):
        copy = pltpu.make_async_remote_copy(
            src_ref=src, dst_ref=dst, send_sem=send_sem, recv_sem=recv_sem,
            device_id=device, device_id_type=MESH,
        )
        copy.start()
        return copy

    def landed(ref, semaphore):
        pltpu.make_async_copy(ref, ref, semaphore).wait()

    def place_rows(i):
        return pl.ds(pl.multiple_of(i * cap, cap), cap)

    my_place = sum(
        ORDER.index(s) * (1 - (lax.rem(z - s + n_ep, n_ep) + n_ep - 1) // n_ep)
        for s in range(n_ep)
    )

    def dispatch(s):
        return pltpu.make_async_remote_copy(
            src_ref=packed.at[s], dst_ref=gathered.at[0, 0, place_rows(my_place), :],
            send_sem=z_send, recv_sem=z_recv.at[z],
            device_id={"ep": s}, device_id_type=MESH,
        )

    for s in sorted(range(n_ep), key=lambda s: -min(s, n_ep - s)):

        @pl.when((s != z) & ((z >= 0) if s < early_count else (z >= early_count)))
        def _():
            dispatch(s).start()

    def dispatch_late(s):
        @pl.when(z < early_count)
        def _():
            pl.semaphore_wait(ready.at[s - early_count], 1)
            dispatch(s).start()

    gathered[0, 0, place_rows(my_place), :] = packed[z]

    small[2].wait()
    mix = sum(
        jnp.where(hit, jnp.broadcast_to(weights[k : k + 1, :], (all_rows, tok_rows)), 0.0)
        for k, hit in enumerate(hits)
    ) * chosen
    mix_high = mix.astype(jnp.bfloat16)
    mix_low = (mix - mix_high.astype(jnp.float32)).astype(jnp.bfloat16)
    unit = (
        lax.broadcasted_iota(jnp.int32, (tok_rows, tok_rows), 0)
        == lax.broadcasted_iota(jnp.int32, (tok_rows, tok_rows), 1)
    ).astype(jnp.float32).astype(jnp.bfloat16)

    def flipped(value):
        return lax.dot_general(
            unit, value, (((1,), (1,)), ((), ())), preferred_element_type=jnp.float32
        ).astype(jnp.bfloat16)

    mix_high, mix_low = flipped(mix_high), flipped(mix_low)

    def span(c):
        return pl.ds(firsts[c], firsts[c + 1] - firsts[c])

    def halved(c):
        return (firsts[c + 1] - firsts[c]) // 2

    def top_half(c):
        return pl.ds(firsts[c], halved(c))

    def low_half(c):
        return pl.ds(firsts[c] + halved(c), halved(c))

    ag, d2d, halves, rs = {}, {}, {}, {}

    def to_sibling(c, d, at, kind):
        d2d[c, kind] = send(
            gathered.at[0, d, at, :], gathered.at[1, d, at, :],
            d2d_send.at[c], d2d_recv.at[c, kind], sibling,
        )

    def gather_own(c):
        for i in range(CUTS[c], CUTS[c + 1]):

            @pl.when(ORDER[i] != z)
            def _():
                landed(gathered.at[0, 0, place_rows(i), :], z_recv.at[ORDER[i]])

        if c in DIRECT:
            hops = [(CHIPS - d, d) for d in far_first]
        else:
            hops = [(2, 6), (6, 2), (1, 7), (7, 1)]
        for slot, d in hops:
            ag[c, slot] = send(
                gathered.at[0, 0, span(c), :], gathered.at[0, slot, span(c), :],
                ag_send.at[c], ag_recv.at[c, slot], at_chip(d),
            )
        to_sibling(c, 0, span(c), 0)

    def share(c):
        for slot in (1, 7, 2, 6, 3, 5, 4):
            ag[c, slot].wait_recv()
            to_sibling(c, slot, span(c), slot)

    def gather_relay(c):
        for slot, near, far, opposite, at, kind in (
            (2, 7, 6, 3, top_half(c), 4),
            (6, 1, 2, 5, low_half(c), 0),
        ):
            ag[c, slot].wait_recv()
            ag[c, kind] = send(
                gathered.at[0, slot, at, :], gathered.at[0, 4, at, :],
                ag_send.at[c], ag_recv.at[c, kind], at_chip(far),
            )
            ag[c, opposite] = send(
                gathered.at[0, slot, span(c), :], gathered.at[0, opposite, span(c), :],
                ag_send.at[c], ag_recv.at[c, opposite], at_chip(near),
            )
            to_sibling(c, slot, span(c), slot)
        for slot in (1, 7):
            ag[c, slot].wait_recv()
            to_sibling(c, slot, span(c), slot)

    def gather_last(c):
        for slot in (3, 5):
            ag[c, slot].wait_recv()
            to_sibling(c, slot, span(c), slot)
        ag[c, 4].wait_recv()
        to_sibling(c, 4, top_half(c), 4)
        ag[c, 0].wait_recv()
        to_sibling(c, 4, low_half(c), 8)

    def feed(c):
        for kind in range(8 if c in DIRECT else 9):
            d2d[c, kind].wait_recv()
        blocks = [(p, d) for p in range(2) for d in range(CHIPS)]
        features = len(blocks) * width
        shape = (firsts[c + 1] - firsts[c], width)
        total = jnp.zeros(shape, jnp.float32)
        for p, d in blocks:
            total += gathered[p, d, span(c), :].astype(jnp.float32)
        average = jnp.sum(total, axis=1, keepdims=True) / features
        total = jnp.zeros(shape, jnp.float32)
        for p, d in blocks:
            off = gathered[p, d, span(c), :].astype(jnp.float32) - average
            total += off * off
        scale = lax.rsqrt(jnp.sum(total, axis=1, keepdims=True) / features + epsilon)
        for p, d in blocks:
            k = p * CHIPS + d
            off = gathered[p, d, span(c), :].astype(jnp.float32) - average
            rows_in[span(c), pl.ds(k * width, width)] = (
                off * scale * gain[pl.ds(owner(p, d), 1), :]
            ).astype(jnp.bfloat16)

    def expert(c):
        both = jnp.dot(rows_in[span(c), :], w_in[...], preferred_element_type=jnp.float32)
        gate_val, up_val = both[:, :hidden_units], both[:, hidden_units:]
        return (gate_val / (1.0 + jnp.exp(-gate_val)) * up_val).astype(jnp.bfloat16)

    def project(c, hidden):
        other = jnp.dot(hidden, w_other[...], preferred_element_type=jnp.float32)
        other = other.astype(jnp.bfloat16)
        for d in range(CHIPS):
            part_out[d, span(c), :] = other[:, d * width : (d + 1) * width]
        halves[c] = send(
            part_out.at[:, span(c), :], part_in.at[:, span(c), :],
            half_send.at[c], half_recv.at[c], sibling,
        )
        own = jnp.dot(hidden, w_own[...], preferred_element_type=jnp.float32)
        for d in range(CHIPS):
            part_own[d, span(c), :] = own[:, d * width : (d + 1) * width]

    def serve(c):
        feed(c)
        project(c, expert(c))

    def chip_part(d, at):
        return part_own[d, at, :] + part_in[d, at, :].astype(jnp.float32)

    def reduce_send(c, kind, d, source, slot, at):
        rs[c, kind] = send(
            sums_out.at[source, at, :], sums_in.at[slot, at, :],
            rs_send.at[c], rs_recv.at[c, kind], at_chip(d),
        )

    def reduce_direct(c):
        halves[c].wait_recv()
        for d in far_first:
            sums_out[d, span(c), :] = chip_part(d, span(c)).astype(jnp.bfloat16)
            reduce_send(c, CHIPS - d, d, d, CHIPS - d, span(c))

    def finish_direct(c):
        value = chip_part(0, span(c))
        for slot in far_first:
            rs[c, slot].wait_recv()
            value += sums_in[slot, span(c), :].astype(jnp.float32)
        give_back(c, value)

    def reduce_first(c):
        halves[c].wait_recv()
        sums_out[4, span(c), :] = chip_part(4, span(c)).astype(jnp.bfloat16)
        reduce_send(c, 4, 2, 4, 4, top_half(c))
        reduce_send(c, 0, 6, 4, 4, low_half(c))
        for d, near in ((3, 1), (5, 7), (1, 1), (7, 7)):
            sums_out[d, span(c), :] = chip_part(d, span(c)).astype(jnp.bfloat16)
            reduce_send(c, d, near, d, d, span(c))

    def reduce_second(c):
        rs[c, 4].wait_recv()
        rs[c, 0].wait_recv()
        for d, near, joined, alone in (
            (2, 3, top_half(c), low_half(c)), (6, 5, low_half(c), top_half(c))
        ):
            rs[c, near].wait_recv()
            sums_out[d, joined, :] = (
                chip_part(d, joined)
                + sums_in[near, joined, :].astype(jnp.float32)
                + sums_in[4, joined, :].astype(jnp.float32)
            ).astype(jnp.bfloat16)
            sums_out[d, alone, :] = (
                chip_part(d, alone) + sums_in[near, alone, :].astype(jnp.float32)
            ).astype(jnp.bfloat16)
            reduce_send(c, d, d, d, d, span(c))

    def finish(c):
        value = chip_part(0, span(c))
        for slot in (1, 7, 2, 6):
            rs[c, slot].wait_recv()
            value += sums_in[slot, span(c), :].astype(jnp.float32)
        give_back(c, value)

    def back(i):
        return pltpu.make_async_remote_copy(
            src_ref=served.at[place_rows(i), :], dst_ref=returned.at[z],
            send_sem=back_send, recv_sem=back_recv.at[z],
            device_id={"ep": ORDER[i]}, device_id_type=MESH,
        )

    def give_back(c, value):
        served[span(c), :] = value.astype(jnp.bfloat16)
        for i in range(CUTS[c], CUTS[c + 1]):

            @pl.when(ORDER[i] != z)
            def _():
                back(i).start()

            @pl.when(ORDER[i] == z)
            def _():
                returned[z] = served[place_rows(i), :]

    late = list(range(n_ep - 1, early_count - 1, -1))
    gather_own(0)
    dispatch_late(late[0])
    gather_own(1)
    dispatch_late(late[1])
    gather_own(2)
    gather_own(3)
    share(0)
    small[3].wait()
    pltpu.make_async_copy(w_in, w_in, in_sem).wait()
    pltpu.make_async_copy(w_other, w_other, other_sem).wait()
    pltpu.make_async_copy(w_own, w_own, own_sem).wait()
    serve(0)
    gather_relay(1)
    reduce_direct(0)
    gather_relay(2)
    gather_relay(3)
    gather_last(1)
    serve(1)
    gather_last(2)
    gather_last(3)
    finish_direct(0)
    reduce_first(1)
    serve(2)
    reduce_first(2)
    serve(3)
    reduce_second(1)
    reduce_first(3)
    reduce_second(2)
    finish(1)
    reduce_second(3)
    finish(2)
    finish(3)

    landed(packed.at[1:], z_send)
    for c in range(CHUNKS):
        landed(gathered.at[0, 1:, span(c), :], ag_send.at[c])
        landed(gathered.at[0, :, span(c), :], d2d_send.at[c])
        landed(part_out.at[:, span(c), :], half_send.at[c])
        landed(sums_out.at[1:, span(c), :], rs_send.at[c])
    for e in range(n_ep):

        @pl.when(e != z)
        def _():
            landed(returned.at[e], back_recv.at[e])

    values = returned[...].reshape(all_rows, width)
    out_ref[...] = (
        jnp.dot(mix_high, values, preferred_element_type=jnp.float32)
        + jnp.dot(mix_low, values, preferred_element_type=jnp.float32)
    ).astype(out_ref.dtype)
    landed(served.at[pl.ds(cap, all_rows - cap), :], back_send)


def solution(mesh):
    n_ep, n_tp = mesh.shape["ep"], mesh.shape["tp"]

    def on_device(tokens, gain, routes, weights, w_gate, w_up, w_down):
        tok_rows, width = tokens.shape
        top = routes.shape[1]
        cap = min(tok_rows, 2 * tok_rows * top // n_ep)
        hidden_units = w_gate.shape[2]
        all_rows = n_ep * cap
        features = n_tp * width
        bf16, f32 = jnp.bfloat16, jnp.float32
        dma = pltpu.SemaphoreType.DMA
        return pl.pallas_call(
            functools.partial(kernel, n_ep, cap),
            out_shape=pltpu.VMEM((tok_rows, width), bf16),
            in_specs=[pl.BlockSpec(memory_space=pltpu.HBM)] * 7,
            out_specs=pl.BlockSpec(memory_space=pltpu.VMEM),
            scratch_shapes=[
                pltpu.VMEM((tok_rows, width), bf16),
                pltpu.VMEM((n_tp, width), f32),
                pltpu.VMEM((top, tok_rows), jnp.int32),
                pltpu.VMEM((top, tok_rows), f32),
                pltpu.VMEM((features, 2 * hidden_units), bf16),
                pltpu.VMEM((hidden_units, features // 2), bf16),
                pltpu.VMEM((hidden_units, features // 2), bf16),
                pltpu.VMEM((n_ep, cap, width), bf16),
                pltpu.VMEM((2, CHIPS, all_rows, width), bf16),
                pltpu.VMEM((all_rows, features), bf16),
                pltpu.VMEM((CHIPS, all_rows, width), f32),
                pltpu.VMEM((CHIPS, all_rows, width), bf16),
                pltpu.VMEM((CHIPS, all_rows, width), bf16),
                pltpu.VMEM((CHIPS, all_rows, width), bf16),
                pltpu.VMEM((CHIPS, all_rows, width), bf16),
                pltpu.VMEM((all_rows, width), bf16),
                pltpu.VMEM((n_ep, cap, width), bf16),
                dma((4,)), dma, dma, dma, pltpu.SemaphoreType.REGULAR((LATE,)),
                dma, dma((n_ep,)),
                dma((CHUNKS,)), dma((CHUNKS, 8)),
                dma((CHUNKS,)), dma((CHUNKS, 9)),
                dma((CHUNKS,)), dma((CHUNKS,)),
                dma((CHUNKS,)), dma((CHUNKS, 8)),
                dma, dma((n_ep,)),
            ],
            compiler_params=pltpu.CompilerParams(collective_id=0, has_side_effects=True),
        )(tokens, gain.reshape(n_tp, width), routes.T, weights.T, w_gate, w_up, w_down)

    in_specs = (
        P(("grp", "ep"), "tp"),
        P(),
        P(("grp", "ep"), None),
        P(("grp", "ep"), None),
        P("ep", None, "tp"),
        P("ep", None, "tp"),
        P("ep", "tp", None),
    )
    out_specs = P(("grp", "ep"), "tp")
    return jax.shard_map(
        on_device, mesh=mesh, in_specs=in_specs, out_specs=out_specs, check_vma=False
    )
```

```python
import functools

import jax
import jax.numpy as jnp
from jax import lax
from jax.experimental import pallas as pl
from jax.experimental.pallas import tpu as pltpu
from jax.sharding import PartitionSpec as P

MESH = pl.DeviceIdType.MESH
epsilon = 1e-05
CHIPS = 8
ORDER = (0, 1, 2, 3, 4, 5, 11, 12, 13, 14, 15, 6, 7, 8, 9, 10)
CUTS = (0, 3, 11, 16)
CHUNKS = len(CUTS) - 1
DIRECT = (0,)
LATE = 1


def kernel(
    n_ep, cap,
    tok_hbm, gain_hbm, routes_hbm, weights_hbm, wg_hbm, wu_hbm, wd_hbm,
    out_ref,
    tok, gain, routes, weights, w_in, w_own, w_other,
    packed, gathered, rows_in, part_own, part_out, part_in, sums_out, sums_in, served, returned,
    small_sem, in_sem, own_sem, other_sem, ready,
    z_send, z_recv, ag_send, ag_recv, d2d_send, d2d_recv, half_send, half_recv,
    rs_send, rs_recv, back_send, back_recv,
):
    z = lax.axis_index("ep")
    tp = lax.axis_index("tp")
    core = lax.rem(tp, 2)
    x = lax.div(tp, 2)
    tok_rows, width = tok.shape
    top = routes.shape[0]
    hidden_units = w_own.shape[0]
    all_rows = n_ep * cap
    firsts = [cut * cap for cut in CUTS]
    early_count = n_ep - LATE
    far_first = sorted(range(1, CHIPS), key=lambda d: -min(d, CHIPS - d))

    def chip(d):
        return lax.rem(x + d, CHIPS)

    chip_at = [chip(d) * 2 + core for d in range(CHIPS)]

    def at_chip(d):
        return {"tp": chip_at[d]}

    sibling = {"tp": x * 2 + 1 - core}

    def owner(p, d):
        return chip(d) * 2 + (core if p == 0 else 1 - core)

    barrier = pltpu.get_barrier_semaphore()

    def greet(device):
        pl.semaphore_signal(barrier, inc=1, device_id=device, device_id_type=MESH)

    far_offsets = sorted(range(1, n_ep), key=lambda o: -min(o, n_ep - o))
    for offset in far_offsets:
        s = lax.rem(z + offset, n_ep)

        @pl.when((z < early_count) | (s >= early_count))
        def _():
            greet({"ep": s})

    for d in far_first:
        greet(at_chip(d))
    greet(sibling)

    @pl.when(z >= early_count)
    def _():
        pl.semaphore_wait(barrier, n_ep - 1 + CHIPS)
        for s in sorted(range(early_count), key=lambda s: min(s, n_ep - s)):
            pl.semaphore_signal(
                ready.at[z - early_count], inc=1, device_id={"ep": s}, device_id_type=MESH
            )

    small = [
        pltpu.make_async_copy(source, target, small_sem.at[i])
        for i, (source, target) in enumerate(
            [(tok_hbm, tok), (routes_hbm, routes), (weights_hbm, weights), (gain_hbm, gain)]
        )
    ]
    for copy in small:
        copy.start()
    small[0].wait()
    small[1].wait()
    place = lax.broadcasted_iota(jnp.int32, (all_rows, tok_rows), 0)
    place_expert = lax.div(place, cap)
    place_turn = lax.rem(place, cap)
    hits = [
        (jnp.broadcast_to(routes[k : k + 1, :], (all_rows, tok_rows)) == place_expert)
        for k in range(top)
    ]
    member = sum(hit.astype(jnp.float32) for hit in hits)
    earlier = (
        lax.broadcasted_iota(jnp.int32, (tok_rows, tok_rows), 0)
        < lax.broadcasted_iota(jnp.int32, (tok_rows, tok_rows), 1)
    ).astype(jnp.float32).astype(jnp.bfloat16)
    turn = jnp.dot(member.astype(jnp.bfloat16), earlier, preferred_element_type=jnp.float32)
    chosen = jnp.where(turn == place_turn.astype(jnp.float32), member, 0.0)
    outbox = jnp.dot(
        chosen.astype(jnp.bfloat16), tok[...], preferred_element_type=jnp.float32
    ).astype(jnp.bfloat16)
    packed[...] = outbox.reshape(n_ep, cap, width)

    @pl.when(z < early_count)
    def _():
        pl.semaphore_wait(barrier, early_count - 1 + CHIPS)

    def send(src, dst, send_sem, recv_sem, device):
        copy = pltpu.make_async_remote_copy(
            src_ref=src, dst_ref=dst, send_sem=send_sem, recv_sem=recv_sem,
            device_id=device, device_id_type=MESH,
        )
        copy.start()
        return copy

    def landed(ref, semaphore):
        pltpu.make_async_copy(ref, ref, semaphore).wait()

    def place_rows(i):
        return pl.ds(pl.multiple_of(i * cap, cap), cap)

    my_place = sum(
        ORDER.index(s) * (1 - (lax.rem(z - s + n_ep, n_ep) + n_ep - 1) // n_ep)
        for s in range(n_ep)
    )

    def dispatch(s):
        return pltpu.make_async_remote_copy(
            src_ref=packed.at[s], dst_ref=gathered.at[0, 0, place_rows(my_place), :],
            send_sem=z_send, recv_sem=z_recv.at[z],
            device_id={"ep": s}, device_id_type=MESH,
        )

    for offset in far_offsets:
        s = lax.rem(z + offset, n_ep)

        @pl.when((z >= early_count) | (s < early_count))
        def _():
            dispatch(s).start()

    def dispatch_late(s):
        @pl.when(z < early_count)
        def _():
            pl.semaphore_wait(ready.at[s - early_count], 1)
            dispatch(s).start()

    gathered[0, 0, place_rows(my_place), :] = packed[z]

    for p in range(2):
        for d in range(CHIPS):
            first = pl.multiple_of(owner(p, d) * width, width)
            k = p * CHIPS + d
            for j, source in enumerate((wg_hbm, wu_hbm)):
                pltpu.make_async_copy(
                    source.at[0, pl.ds(first, width), :],
                    w_in.at[pl.ds(k * width, width), pl.ds(j * hidden_units, hidden_units)],
                    in_sem,
                ).start()
    for p, target, sem in ((1, w_other, other_sem), (0, w_own, own_sem)):
        for d in range(CHIPS):
            first = pl.multiple_of(owner(p, d) * width, width)
            pltpu.make_async_copy(
                wd_hbm.at[0, :, pl.ds(first, width)], target.at[:, pl.ds(d * width, width)], sem
            ).start()

    small[2].wait()
    mix = sum(
        jnp.where(hit, jnp.broadcast_to(weights[k : k + 1, :], (all_rows, tok_rows)), 0.0)
        for k, hit in enumerate(hits)
    ) * chosen
    mix_high = mix.astype(jnp.bfloat16)
    mix_low = (mix - mix_high.astype(jnp.float32)).astype(jnp.bfloat16)
    unit = (
        lax.broadcasted_iota(jnp.int32, (tok_rows, tok_rows), 0)
        == lax.broadcasted_iota(jnp.int32, (tok_rows, tok_rows), 1)
    ).astype(jnp.float32).astype(jnp.bfloat16)

    def flipped(value):
        return lax.dot_general(
            unit, value, (((1,), (1,)), ((), ())), preferred_element_type=jnp.float32
        ).astype(jnp.bfloat16)

    mix_high, mix_low = flipped(mix_high), flipped(mix_low)

    def span(c):
        return pl.ds(firsts[c], firsts[c + 1] - firsts[c])

    def halved(c):
        return ((CUTS[c + 1] - CUTS[c] + 1) // 2) * cap

    def top_half(c):
        return pl.ds(firsts[c], halved(c))

    def low_half(c):
        return pl.ds(firsts[c] + halved(c), firsts[c + 1] - firsts[c] - halved(c))

    ag, d2d, halves = {}, {}, {}

    def to_sibling(c, d, at, kind):
        d2d[c, kind] = send(
            gathered.at[0, d, at, :], gathered.at[1, d, at, :],
            d2d_send.at[c], d2d_recv.at[c, kind], sibling,
        )

    def gather_own(c):
        for i in range(CUTS[c], CUTS[c + 1]):

            @pl.when(ORDER[i] != z)
            def _():
                landed(gathered.at[0, 0, place_rows(i), :], z_recv.at[ORDER[i]])

        if c in DIRECT:
            hops = [(CHIPS - d, d) for d in far_first]
        else:
            hops = [(2, 6), (6, 2), (1, 7), (7, 1)]
        for slot, d in hops:
            ag[c, slot] = send(
                gathered.at[0, 0, span(c), :], gathered.at[0, slot, span(c), :],
                ag_send.at[c], ag_recv.at[c, slot], at_chip(d),
            )
        to_sibling(c, 0, span(c), 0)

    def share(c):
        for slot in (1, 7, 2, 6, 3, 5, 4):
            ag[c, slot].wait_recv()
            to_sibling(c, slot, span(c), slot)

    def gather_relay(c):
        for slot, near, far, opposite, at, kind in (
            (2, 7, 6, 3, top_half(c), 4),
            (6, 1, 2, 5, low_half(c), 0),
        ):
            ag[c, slot].wait_recv()
            ag[c, kind] = send(
                gathered.at[0, slot, at, :], gathered.at[0, 4, at, :],
                ag_send.at[c], ag_recv.at[c, kind], at_chip(far),
            )
            ag[c, opposite] = send(
                gathered.at[0, slot, span(c), :], gathered.at[0, opposite, span(c), :],
                ag_send.at[c], ag_recv.at[c, opposite], at_chip(near),
            )
            to_sibling(c, slot, span(c), slot)
        for slot in (1, 7):
            ag[c, slot].wait_recv()
            to_sibling(c, slot, span(c), slot)

    def gather_last(c):
        for slot in (3, 5):
            ag[c, slot].wait_recv()
            to_sibling(c, slot, span(c), slot)
        ag[c, 4].wait_recv()
        to_sibling(c, 4, top_half(c), 4)
        ag[c, 0].wait_recv()
        to_sibling(c, 4, low_half(c), 8)

    def feed(c):
        for kind in range(8 if c in DIRECT else 9):
            d2d[c, kind].wait_recv()
        blocks = [(p, d) for p in range(2) for d in range(CHIPS)]
        features = len(blocks) * width
        shape = (firsts[c + 1] - firsts[c], width)
        total = jnp.zeros(shape, jnp.float32)
        for p, d in blocks:
            total += gathered[p, d, span(c), :].astype(jnp.float32)
        average = jnp.sum(total, axis=1, keepdims=True) / features
        total = jnp.zeros(shape, jnp.float32)
        for p, d in blocks:
            off = gathered[p, d, span(c), :].astype(jnp.float32) - average
            total += off * off
        scale = lax.rsqrt(jnp.sum(total, axis=1, keepdims=True) / features + epsilon)
        for p, d in blocks:
            k = p * CHIPS + d
            off = gathered[p, d, span(c), :].astype(jnp.float32) - average
            rows_in[span(c), pl.ds(k * width, width)] = (
                off * scale * gain[pl.ds(owner(p, d), 1), :]
            ).astype(jnp.bfloat16)

    def expert(c):
        both = jnp.dot(rows_in[span(c), :], w_in[...], preferred_element_type=jnp.float32)
        gate_val, up_val = both[:, :hidden_units], both[:, hidden_units:]
        return (gate_val / (1.0 + jnp.exp(-gate_val)) * up_val).astype(jnp.bfloat16)

    def project(c, hidden):
        other = jnp.dot(hidden, w_other[...], preferred_element_type=jnp.float32)
        other = other.astype(jnp.bfloat16)
        for d in range(CHIPS):
            part_out[d, span(c), :] = other[:, d * width : (d + 1) * width]
        halves[c] = send(
            part_out.at[:, span(c), :], part_in.at[:, span(c), :],
            half_send.at[c], half_recv.at[c], sibling,
        )
        own = jnp.dot(hidden, w_own[...], preferred_element_type=jnp.float32)
        for d in range(CHIPS):
            part_own[d, span(c), :] = own[:, d * width : (d + 1) * width]

    def serve(c):
        feed(c)
        project(c, expert(c))

    def chip_part(d, at):
        return part_own[d, at, :] + part_in[d, at, :].astype(jnp.float32)

    def reduce_send(c, kind, d, source, slot, at):
        send(
            sums_out.at[source, at, :], sums_in.at[slot, at, :],
            rs_send.at[c], rs_recv.at[c, kind], at_chip(d),
        )

    def reduced(c, kind, at):
        landed(sums_in.at[kind or 4, at, :], rs_recv.at[c, kind])

    def reduce_direct(c):
        halves[c].wait_recv()
        for d in far_first:
            sums_out[d, span(c), :] = chip_part(d, span(c)).astype(jnp.bfloat16)
            reduce_send(c, CHIPS - d, d, d, CHIPS - d, span(c))

    def finish_direct(c):
        value = chip_part(0, span(c))
        for slot in far_first:
            reduced(c, slot, span(c))
            value += sums_in[slot, span(c), :].astype(jnp.float32)
        give_back(c, value)

    def reduce_first(c):
        halves[c].wait_recv()
        sums_out[4, span(c), :] = chip_part(4, span(c)).astype(jnp.bfloat16)
        reduce_send(c, 4, 2, 4, 4, top_half(c))
        reduce_send(c, 0, 6, 4, 4, low_half(c))
        for d, near in ((3, 1), (5, 7), (1, 1), (7, 7)):
            sums_out[d, span(c), :] = chip_part(d, span(c)).astype(jnp.bfloat16)
            reduce_send(c, d, near, d, d, span(c))

    def reduce_second(c):
        reduced(c, 4, top_half(c))
        reduced(c, 0, low_half(c))
        for d, near, joined, alone in (
            (2, 3, top_half(c), low_half(c)), (6, 5, low_half(c), top_half(c))
        ):
            reduced(c, near, span(c))
            sums_out[d, joined, :] = (
                chip_part(d, joined)
                + sums_in[near, joined, :].astype(jnp.float32)
                + sums_in[4, joined, :].astype(jnp.float32)
            ).astype(jnp.bfloat16)
            sums_out[d, alone, :] = (
                chip_part(d, alone) + sums_in[near, alone, :].astype(jnp.float32)
            ).astype(jnp.bfloat16)
            reduce_send(c, d, d, d, d, span(c))

    def finish(c):
        value = chip_part(0, span(c))
        for slot in (1, 7, 2, 6):
            reduced(c, slot, span(c))
            value += sums_in[slot, span(c), :].astype(jnp.float32)
        give_back(c, value)

    def back(i):
        return pltpu.make_async_remote_copy(
            src_ref=served.at[place_rows(i), :], dst_ref=returned.at[z],
            send_sem=back_send, recv_sem=back_recv.at[z],
            device_id={"ep": ORDER[i]}, device_id_type=MESH,
        )

    def give_back(c, value):
        served[span(c), :] = value.astype(jnp.bfloat16)
        for i in range(CUTS[c], CUTS[c + 1]):

            @pl.when(ORDER[i] != z)
            def _():
                back(i).start()

            @pl.when(ORDER[i] == z)
            def _():
                returned[z] = served[place_rows(i), :]

    gather_own(0)
    for s in range(n_ep - 1, early_count - 1, -1):
        dispatch_late(s)
    gather_own(1)
    share(0)
    gather_own(2)
    small[3].wait()
    pltpu.make_async_copy(w_in, w_in, in_sem).wait()
    pltpu.make_async_copy(w_other, w_other, other_sem).wait()
    pltpu.make_async_copy(w_own, w_own, own_sem).wait()
    serve(0)
    gather_relay(1)
    reduce_direct(0)
    gather_relay(2)
    gather_last(1)
    serve(1)
    finish_direct(0)
    gather_last(2)
    pl.when(core == 1)(lambda: reduce_first(1))
    serve(2)
    pl.when(core == 0)(lambda: reduce_first(1))
    reduce_first(2)
    reduce_second(1)
    reduce_second(2)
    finish(1)
    finish(2)

    landed(packed.at[1:], z_send)
    for c in range(CHUNKS):
        landed(gathered.at[0, 1:, span(c), :], ag_send.at[c])
        landed(gathered.at[0, :, span(c), :], d2d_send.at[c])
        landed(part_out.at[:, span(c), :], half_send.at[c])
        landed(sums_out.at[1:, span(c), :], rs_send.at[c])
    for e in range(n_ep):

        @pl.when(e != z)
        def _():
            landed(returned.at[e], back_recv.at[e])

    values = returned[...].reshape(all_rows, width)
    out_ref[...] = (
        jnp.dot(mix_high, values, preferred_element_type=jnp.float32)
        + jnp.dot(mix_low, values, preferred_element_type=jnp.float32)
    ).astype(out_ref.dtype)
    landed(served.at[pl.ds(cap, all_rows - cap), :], back_send)


def solution(mesh):
    n_ep, n_tp = mesh.shape["ep"], mesh.shape["tp"]

    def on_device(tokens, gain, routes, weights, w_gate, w_up, w_down):
        tok_rows, width = tokens.shape
        top = routes.shape[1]
        cap = min(tok_rows, 2 * tok_rows * top // n_ep)
        hidden_units = w_gate.shape[2]
        all_rows = n_ep * cap
        features = n_tp * width
        bf16, f32 = jnp.bfloat16, jnp.float32
        dma = pltpu.SemaphoreType.DMA
        return pl.pallas_call(
            functools.partial(kernel, n_ep, cap),
            out_shape=pltpu.VMEM((tok_rows, width), bf16),
            in_specs=[pl.BlockSpec(memory_space=pltpu.HBM)] * 7,
            out_specs=pl.BlockSpec(memory_space=pltpu.VMEM),
            scratch_shapes=[
                pltpu.VMEM((tok_rows, width), bf16),
                pltpu.VMEM((n_tp, width), f32),
                pltpu.VMEM((top, tok_rows), jnp.int32),
                pltpu.VMEM((top, tok_rows), f32),
                pltpu.VMEM((features, 2 * hidden_units), bf16),
                pltpu.VMEM((hidden_units, features // 2), bf16),
                pltpu.VMEM((hidden_units, features // 2), bf16),
                pltpu.VMEM((n_ep, cap, width), bf16),
                pltpu.VMEM((2, CHIPS, all_rows, width), bf16),
                pltpu.VMEM((all_rows, features), bf16),
                pltpu.VMEM((CHIPS, all_rows, width), f32),
                pltpu.VMEM((CHIPS, all_rows, width), bf16),
                pltpu.VMEM((CHIPS, all_rows, width), bf16),
                pltpu.VMEM((CHIPS, all_rows, width), bf16),
                pltpu.VMEM((CHIPS, all_rows, width), bf16),
                pltpu.VMEM((all_rows, width), bf16),
                pltpu.VMEM((n_ep, cap, width), bf16),
                dma((4,)), dma, dma, dma, pltpu.SemaphoreType.REGULAR((LATE,)),
                dma, dma((n_ep,)),
                dma((CHUNKS,)), dma((CHUNKS, 8)),
                dma((CHUNKS,)), dma((CHUNKS, 9)),
                dma((CHUNKS,)), dma((CHUNKS,)),
                dma((CHUNKS,)), dma((CHUNKS, 8)),
                dma, dma((n_ep,)),
            ],
            compiler_params=pltpu.CompilerParams(collective_id=0, has_side_effects=True),
        )(tokens, gain.reshape(n_tp, width), routes.T, weights.T, w_gate, w_up, w_down)

    in_specs = (
        P(("grp", "ep"), "tp"),
        P(),
        P(("grp", "ep"), None),
        P(("grp", "ep"), None),
        P("ep", None, "tp"),
        P("ep", None, "tp"),
        P("ep", "tp", None),
    )
    out_specs = P(("grp", "ep"), "tp")
    return jax.shard_map(
        on_device, mesh=mesh, in_specs=in_specs, out_specs=out_specs, check_vma=False
    )
```

```python
import functools

import jax
import jax.numpy as jnp
from jax import lax
from jax.experimental import pallas as pl
from jax.experimental.pallas import tpu as pltpu
from jax.sharding import PartitionSpec as P

MESH = pl.DeviceIdType.MESH
epsilon = 1e-05
CHIPS = 8
ORDER = (0, 1, 2, 3, 4, 11, 12, 13, 14, 5, 6, 7, 8, 9, 10, 15)
CUTS = (0, 3, 9, 16)
CHUNKS = len(CUTS) - 1
DIRECT = (0,)
LATE = 1


def kernel(
    n_ep, cap,
    tok_hbm, gain_hbm, routes_hbm, weights_hbm, wg_hbm, wu_hbm, wd_hbm,
    out_ref,
    tok, gain, routes, weights, w_in, w_own, w_other,
    packed, gathered, rows_in, part_own, part_out, part_in, sums_out, sums_in, served, returned,
    small_sem, in_sem, own_sem, other_sem, ready,
    z_send, z_recv, ag_send, ag_recv, d2d_send, d2d_recv, half_send, half_recv,
    rs_send, rs_recv, back_send, back_recv,
):
    z = lax.axis_index("ep")
    tp = lax.axis_index("tp")
    core = lax.rem(tp, 2)
    x = lax.div(tp, 2)
    tok_rows, width = tok.shape
    top = routes.shape[0]
    hidden_units = w_own.shape[0]
    all_rows = n_ep * cap
    firsts = [cut * cap for cut in CUTS]
    early_count = n_ep - LATE
    far_first = sorted(range(1, CHIPS), key=lambda d: -min(d, CHIPS - d))

    def chip(d):
        return lax.rem(x + d, CHIPS)

    chip_at = [chip(d) * 2 + core for d in range(CHIPS)]

    def at_chip(d):
        return {"tp": chip_at[d]}

    sibling = {"tp": x * 2 + 1 - core}

    def owner(p, d):
        return chip(d) * 2 + (core if p == 0 else 1 - core)

    barrier = pltpu.get_barrier_semaphore()

    def greet(device):
        pl.semaphore_signal(barrier, inc=1, device_id=device, device_id_type=MESH)

    far_offsets = sorted(range(1, n_ep), key=lambda o: -min(o, n_ep - o))
    for offset in far_offsets:
        s = lax.rem(z + offset, n_ep)

        @pl.when((z < early_count) | (s >= early_count))
        def _():
            greet({"ep": s})

    for d in far_first:
        greet(at_chip(d))
    greet(sibling)

    @pl.when(z >= early_count)
    def _():
        pl.semaphore_wait(barrier, n_ep - 1 + CHIPS)
        for s in sorted(range(early_count), key=lambda s: min(s, n_ep - s)):
            pl.semaphore_signal(
                ready.at[z - early_count], inc=1, device_id={"ep": s}, device_id_type=MESH
            )

    small = [
        pltpu.make_async_copy(source, target, small_sem.at[i])
        for i, (source, target) in enumerate(
            [(tok_hbm, tok), (routes_hbm, routes), (weights_hbm, weights), (gain_hbm, gain)]
        )
    ]
    for copy in small:
        copy.start()
    small[0].wait()
    small[1].wait()
    place = lax.broadcasted_iota(jnp.int32, (all_rows, tok_rows), 0)
    place_expert = lax.div(place, cap)
    place_turn = lax.rem(place, cap)
    hits = [
        (jnp.broadcast_to(routes[k : k + 1, :], (all_rows, tok_rows)) == place_expert)
        for k in range(top)
    ]
    member = sum(hit.astype(jnp.float32) for hit in hits)
    earlier = (
        lax.broadcasted_iota(jnp.int32, (tok_rows, tok_rows), 0)
        < lax.broadcasted_iota(jnp.int32, (tok_rows, tok_rows), 1)
    ).astype(jnp.float32).astype(jnp.bfloat16)
    turn = jnp.dot(member.astype(jnp.bfloat16), earlier, preferred_element_type=jnp.float32)
    chosen = jnp.where(turn == place_turn.astype(jnp.float32), member, 0.0)
    outbox = jnp.dot(
        chosen.astype(jnp.bfloat16), tok[...], preferred_element_type=jnp.float32
    ).astype(jnp.bfloat16)
    packed[...] = outbox.reshape(n_ep, cap, width)

    @pl.when(z < early_count)
    def _():
        pl.semaphore_wait(barrier, early_count - 1 + CHIPS)

    def send(src, dst, send_sem, recv_sem, device):
        copy = pltpu.make_async_remote_copy(
            src_ref=src, dst_ref=dst, send_sem=send_sem, recv_sem=recv_sem,
            device_id=device, device_id_type=MESH,
        )
        copy.start()
        return copy

    def landed(ref, semaphore):
        pltpu.make_async_copy(ref, ref, semaphore).wait()

    def place_rows(i):
        return pl.ds(pl.multiple_of(i * cap, cap), cap)

    my_place = sum(
        ORDER.index(s) * (1 - (lax.rem(z - s + n_ep, n_ep) + n_ep - 1) // n_ep)
        for s in range(n_ep)
    )

    def dispatch(s):
        return pltpu.make_async_remote_copy(
            src_ref=packed.at[s], dst_ref=gathered.at[0, 0, place_rows(my_place), :],
            send_sem=z_send, recv_sem=z_recv.at[z],
            device_id={"ep": s}, device_id_type=MESH,
        )

    for offset in far_offsets:
        s = lax.rem(z + offset, n_ep)

        @pl.when((z >= early_count) | (s < early_count))
        def _():
            dispatch(s).start()

    def dispatch_late(s):
        @pl.when(z < early_count)
        def _():
            pl.semaphore_wait(ready.at[s - early_count], 1)
            dispatch(s).start()

    gathered[0, 0, place_rows(my_place), :] = packed[z]

    for p in range(2):
        for d in range(CHIPS):
            first = pl.multiple_of(owner(p, d) * width, width)
            k = p * CHIPS + d
            for j, source in enumerate((wg_hbm, wu_hbm)):
                pltpu.make_async_copy(
                    source.at[0, pl.ds(first, width), :],
                    w_in.at[pl.ds(k * width, width), pl.ds(j * hidden_units, hidden_units)],
                    in_sem,
                ).start()
    for p, target, sem in ((1, w_other, other_sem), (0, w_own, own_sem)):
        for d in range(CHIPS):
            first = pl.multiple_of(owner(p, d) * width, width)
            pltpu.make_async_copy(
                wd_hbm.at[0, :, pl.ds(first, width)], target.at[:, pl.ds(d * width, width)], sem
            ).start()

    small[2].wait()
    mix = sum(
        jnp.where(hit, jnp.broadcast_to(weights[k : k + 1, :], (all_rows, tok_rows)), 0.0)
        for k, hit in enumerate(hits)
    ) * chosen
    mix_high = mix.astype(jnp.bfloat16)
    mix_low = (mix - mix_high.astype(jnp.float32)).astype(jnp.bfloat16)
    unit = (
        lax.broadcasted_iota(jnp.int32, (tok_rows, tok_rows), 0)
        == lax.broadcasted_iota(jnp.int32, (tok_rows, tok_rows), 1)
    ).astype(jnp.float32).astype(jnp.bfloat16)

    def flipped(value):
        return lax.dot_general(
            unit, value, (((1,), (1,)), ((), ())), preferred_element_type=jnp.float32
        ).astype(jnp.bfloat16)

    mix_high, mix_low = flipped(mix_high), flipped(mix_low)

    def span(c):
        return pl.ds(firsts[c], firsts[c + 1] - firsts[c])

    def halved(c):
        return ((CUTS[c + 1] - CUTS[c] + 1) // 2) * cap

    def top_half(c):
        return pl.ds(firsts[c], halved(c))

    def low_half(c):
        return pl.ds(firsts[c] + halved(c), firsts[c + 1] - firsts[c] - halved(c))

    ag, d2d, halves = {}, {}, {}

    def to_sibling(c, d, at, kind):
        d2d[c, kind] = send(
            gathered.at[0, d, at, :], gathered.at[1, d, at, :],
            d2d_send.at[c], d2d_recv.at[c, kind], sibling,
        )

    def gather_own(c):
        for i in range(CUTS[c], CUTS[c + 1]):

            @pl.when(ORDER[i] != z)
            def _():
                landed(gathered.at[0, 0, place_rows(i), :], z_recv.at[ORDER[i]])

        if c in DIRECT:
            hops = [(CHIPS - d, d) for d in far_first]
        else:
            hops = [(2, 6), (6, 2), (1, 7), (7, 1)]
        for slot, d in hops:
            ag[c, slot] = send(
                gathered.at[0, 0, span(c), :], gathered.at[0, slot, span(c), :],
                ag_send.at[c], ag_recv.at[c, slot], at_chip(d),
            )
        to_sibling(c, 0, span(c), 0)

    def share(c):
        for slot in (1, 7, 2, 6, 3, 5, 4):
            ag[c, slot].wait_recv()
            to_sibling(c, slot, span(c), slot)

    def gather_relay(c):
        for slot, near, far, opposite, at, kind in (
            (2, 7, 6, 3, top_half(c), 4),
            (6, 1, 2, 5, low_half(c), 0),
        ):
            ag[c, slot].wait_recv()
            ag[c, kind] = send(
                gathered.at[0, slot, at, :], gathered.at[0, 4, at, :],
                ag_send.at[c], ag_recv.at[c, kind], at_chip(far),
            )
            ag[c, opposite] = send(
                gathered.at[0, slot, span(c), :], gathered.at[0, opposite, span(c), :],
                ag_send.at[c], ag_recv.at[c, opposite], at_chip(near),
            )
            to_sibling(c, slot, span(c), slot)
        for slot in (1, 7):
            ag[c, slot].wait_recv()
            to_sibling(c, slot, span(c), slot)

    def gather_last(c):
        for slot in (3, 5):
            ag[c, slot].wait_recv()
            to_sibling(c, slot, span(c), slot)
        ag[c, 4].wait_recv()
        to_sibling(c, 4, top_half(c), 4)
        ag[c, 0].wait_recv()
        to_sibling(c, 4, low_half(c), 8)

    def feed(c):
        for kind in range(8 if c in DIRECT else 9):
            d2d[c, kind].wait_recv()
        blocks = [(p, d) for p in range(2) for d in range(CHIPS)]
        features = len(blocks) * width
        shape = (firsts[c + 1] - firsts[c], width)
        total = jnp.zeros(shape, jnp.float32)
        for p, d in blocks:
            total += gathered[p, d, span(c), :].astype(jnp.float32)
        average = jnp.sum(total, axis=1, keepdims=True) / features
        total = jnp.zeros(shape, jnp.float32)
        for p, d in blocks:
            off = gathered[p, d, span(c), :].astype(jnp.float32) - average
            total += off * off
        scale = lax.rsqrt(jnp.sum(total, axis=1, keepdims=True) / features + epsilon)
        for p, d in blocks:
            k = p * CHIPS + d
            off = gathered[p, d, span(c), :].astype(jnp.float32) - average
            rows_in[span(c), pl.ds(k * width, width)] = (
                off * scale * gain[pl.ds(owner(p, d), 1), :]
            ).astype(jnp.bfloat16)

    def expert(c):
        both = jnp.dot(rows_in[span(c), :], w_in[...], preferred_element_type=jnp.float32)
        gate_val, up_val = both[:, :hidden_units], both[:, hidden_units:]
        return (gate_val / (1.0 + jnp.exp(-gate_val)) * up_val).astype(jnp.bfloat16)

    def project(c, hidden):
        other = jnp.dot(hidden, w_other[...], preferred_element_type=jnp.float32)
        other = other.astype(jnp.bfloat16)
        for d in range(CHIPS):
            part_out[d, span(c), :] = other[:, d * width : (d + 1) * width]
        halves[c] = send(
            part_out.at[:, span(c), :], part_in.at[:, span(c), :],
            half_send.at[c], half_recv.at[c], sibling,
        )
        own = jnp.dot(hidden, w_own[...], preferred_element_type=jnp.float32)
        for d in range(CHIPS):
            part_own[d, span(c), :] = own[:, d * width : (d + 1) * width]

    def serve(c):
        feed(c)
        project(c, expert(c))

    def chip_part(d, at):
        return part_own[d, at, :] + part_in[d, at, :].astype(jnp.float32)

    def reduce_send(c, kind, d, source, slot, at):
        send(
            sums_out.at[source, at, :], sums_in.at[slot, at, :],
            rs_send.at[c], rs_recv.at[c, kind], at_chip(d),
        )

    def reduced(c, kind, at):
        landed(sums_in.at[kind or 4, at, :], rs_recv.at[c, kind])

    def reduce_direct(c):
        halves[c].wait_recv()
        for d in far_first:
            sums_out[d, span(c), :] = chip_part(d, span(c)).astype(jnp.bfloat16)
            reduce_send(c, CHIPS - d, d, d, CHIPS - d, span(c))

    def finish_direct(c):
        value = chip_part(0, span(c))
        for slot in far_first:
            reduced(c, slot, span(c))
            value += sums_in[slot, span(c), :].astype(jnp.float32)
        give_back(c, value)

    def reduce_first(c):
        halves[c].wait_recv()
        sums_out[4, span(c), :] = chip_part(4, span(c)).astype(jnp.bfloat16)
        reduce_send(c, 4, 2, 4, 4, top_half(c))
        reduce_send(c, 0, 6, 4, 4, low_half(c))
        for d, near in ((3, 1), (5, 7), (1, 1), (7, 7)):
            sums_out[d, span(c), :] = chip_part(d, span(c)).astype(jnp.bfloat16)
            reduce_send(c, d, near, d, d, span(c))

    def reduce_second(c):
        reduced(c, 4, top_half(c))
        reduced(c, 0, low_half(c))
        for d, near, joined, alone in (
            (2, 3, top_half(c), low_half(c)), (6, 5, low_half(c), top_half(c))
        ):
            reduced(c, near, span(c))
            sums_out[d, joined, :] = (
                chip_part(d, joined)
                + sums_in[near, joined, :].astype(jnp.float32)
                + sums_in[4, joined, :].astype(jnp.float32)
            ).astype(jnp.bfloat16)
            sums_out[d, alone, :] = (
                chip_part(d, alone) + sums_in[near, alone, :].astype(jnp.float32)
            ).astype(jnp.bfloat16)
            reduce_send(c, d, d, d, d, span(c))

    def finish(c):
        value = chip_part(0, span(c))
        for slot in (1, 7, 2, 6):
            reduced(c, slot, span(c))
            value += sums_in[slot, span(c), :].astype(jnp.float32)
        give_back(c, value)

    def back(i):
        return pltpu.make_async_remote_copy(
            src_ref=served.at[place_rows(i), :], dst_ref=returned.at[z],
            send_sem=back_send, recv_sem=back_recv.at[z],
            device_id={"ep": ORDER[i]}, device_id_type=MESH,
        )

    def give_back(c, value):
        served[span(c), :] = value.astype(jnp.bfloat16)
        for i in range(CUTS[c], CUTS[c + 1]):

            @pl.when(ORDER[i] != z)
            def _():
                back(i).start()

            @pl.when(ORDER[i] == z)
            def _():
                returned[z] = served[place_rows(i), :]

    gather_own(0)
    for s in range(n_ep - 1, early_count - 1, -1):
        dispatch_late(s)
    gather_own(1)
    share(0)
    gather_own(2)
    small[3].wait()
    pltpu.make_async_copy(w_in, w_in, in_sem).wait()
    pltpu.make_async_copy(w_other, w_other, other_sem).wait()
    pltpu.make_async_copy(w_own, w_own, own_sem).wait()
    gather_relay(1)
    serve(0)
    reduce_direct(0)
    gather_relay(2)
    gather_last(1)
    serve(1)
    finish_direct(0)
    gather_last(2)
    reduce_first(1)
    serve(2)
    reduce_first(2)
    reduce_second(1)
    reduce_second(2)
    finish(1)
    finish(2)

    landed(packed.at[1:], z_send)
    for c in range(CHUNKS):
        landed(gathered.at[0, 1:, span(c), :], ag_send.at[c])
        landed(gathered.at[0, :, span(c), :], d2d_send.at[c])
        landed(part_out.at[:, span(c), :], half_send.at[c])
        landed(sums_out.at[1:, span(c), :], rs_send.at[c])
    for e in range(n_ep):

        @pl.when(e != z)
        def _():
            landed(returned.at[e], back_recv.at[e])

    values = returned[...].reshape(all_rows, width)
    out_ref[...] = (
        jnp.dot(mix_high, values, preferred_element_type=jnp.float32)
        + jnp.dot(mix_low, values, preferred_element_type=jnp.float32)
    ).astype(out_ref.dtype)
    landed(served.at[pl.ds(cap, all_rows - cap), :], back_send)


def solution(mesh):
    n_ep, n_tp = mesh.shape["ep"], mesh.shape["tp"]

    def on_device(tokens, gain, routes, weights, w_gate, w_up, w_down):
        tok_rows, width = tokens.shape
        top = routes.shape[1]
        cap = min(tok_rows, 2 * tok_rows * top // n_ep)
        hidden_units = w_gate.shape[2]
        all_rows = n_ep * cap
        features = n_tp * width
        bf16, f32 = jnp.bfloat16, jnp.float32
        dma = pltpu.SemaphoreType.DMA
        return pl.pallas_call(
            functools.partial(kernel, n_ep, cap),
            out_shape=pltpu.VMEM((tok_rows, width), bf16),
            in_specs=[pl.BlockSpec(memory_space=pltpu.HBM)] * 7,
            out_specs=pl.BlockSpec(memory_space=pltpu.VMEM),
            scratch_shapes=[
                pltpu.VMEM((tok_rows, width), bf16),
                pltpu.VMEM((n_tp, width), f32),
                pltpu.VMEM((top, tok_rows), jnp.int32),
                pltpu.VMEM((top, tok_rows), f32),
                pltpu.VMEM((features, 2 * hidden_units), bf16),
                pltpu.VMEM((hidden_units, features // 2), bf16),
                pltpu.VMEM((hidden_units, features // 2), bf16),
                pltpu.VMEM((n_ep, cap, width), bf16),
                pltpu.VMEM((2, CHIPS, all_rows, width), bf16),
                pltpu.VMEM((all_rows, features), bf16),
                pltpu.VMEM((CHIPS, all_rows, width), f32),
                pltpu.VMEM((CHIPS, all_rows, width), bf16),
                pltpu.VMEM((CHIPS, all_rows, width), bf16),
                pltpu.VMEM((CHIPS, all_rows, width), bf16),
                pltpu.VMEM((CHIPS, all_rows, width), bf16),
                pltpu.VMEM((all_rows, width), bf16),
                pltpu.VMEM((n_ep, cap, width), bf16),
                dma((4,)), dma, dma, dma, pltpu.SemaphoreType.REGULAR((LATE,)),
                dma, dma((n_ep,)),
                dma((CHUNKS,)), dma((CHUNKS, 8)),
                dma((CHUNKS,)), dma((CHUNKS, 9)),
                dma((CHUNKS,)), dma((CHUNKS,)),
                dma((CHUNKS,)), dma((CHUNKS, 8)),
                dma, dma((n_ep,)),
            ],
            compiler_params=pltpu.CompilerParams(collective_id=0, has_side_effects=True),
        )(tokens, gain.reshape(n_tp, width), routes.T, weights.T, w_gate, w_up, w_down)

    in_specs = (
        P(("grp", "ep"), "tp"),
        P(),
        P(("grp", "ep"), None),
        P(("grp", "ep"), None),
        P("ep", None, "tp"),
        P("ep", None, "tp"),
        P("ep", "tp", None),
    )
    out_specs = P(("grp", "ep"), "tp")
    return jax.shard_map(
        on_device, mesh=mesh, in_specs=in_specs, out_specs=out_specs, check_vma=False
    )
```

```python
import functools

import jax
import jax.numpy as jnp
from jax import lax
from jax.experimental import pallas as pl
from jax.experimental.pallas import tpu as pltpu
from jax.sharding import PartitionSpec as P

MESH = pl.DeviceIdType.MESH
epsilon = 1e-05
CHIPS = 8
ORDER = (0, 1, 2, 3, 4, 11, 12, 13, 14, 5, 6, 7, 8, 9, 10, 15)
CUTS = (0, 3, 9, 16)
CHUNKS = len(CUTS) - 1
DIRECT = (0,)
LATE = 2


def kernel(
    n_ep, cap,
    tok_hbm, gain_hbm, routes_hbm, weights_hbm, wg_hbm, wu_hbm, wd_hbm,
    out_ref,
    tok, gain, routes, weights, w_in, w_own, w_other,
    packed, gathered, rows_in, part_own, part_out, part_in, sums_out, sums_in, served, returned,
    small_sem, in_sem, own_sem, other_sem, ready,
    z_send, z_recv, ag_send, ag_recv, d2d_send, d2d_recv, half_send, half_recv,
    rs_send, rs_recv, back_send, back_recv,
):
    z = lax.axis_index("ep")
    tp = lax.axis_index("tp")
    core = lax.rem(tp, 2)
    x = lax.div(tp, 2)
    tok_rows, width = tok.shape
    top = routes.shape[0]
    hidden_units = w_own.shape[0]
    all_rows = n_ep * cap
    firsts = [cut * cap for cut in CUTS]
    early_count = n_ep - LATE
    far_first = sorted(range(1, CHIPS), key=lambda d: -min(d, CHIPS - d))

    def chip(d):
        return lax.rem(x + d, CHIPS)

    chip_at = [chip(d) * 2 + core for d in range(CHIPS)]

    def at_chip(d):
        return {"tp": chip_at[d]}

    sibling = {"tp": x * 2 + 1 - core}

    def owner(p, d):
        return chip(d) * 2 + (core if p == 0 else 1 - core)

    barrier = pltpu.get_barrier_semaphore()

    def greet(device):
        pl.semaphore_signal(barrier, inc=1, device_id=device, device_id_type=MESH)

    far_offsets = sorted(range(1, n_ep), key=lambda o: -min(o, n_ep - o))
    for offset in far_offsets:
        s = lax.rem(z + offset, n_ep)

        @pl.when((z < early_count) | (s >= early_count))
        def _():
            greet({"ep": s})

    for d in far_first:
        greet(at_chip(d))
    greet(sibling)

    @pl.when(z >= early_count)
    def _():
        pl.semaphore_wait(barrier, n_ep - 1 + CHIPS)
        for s in sorted(range(early_count), key=lambda s: min(s, n_ep - s)):
            pl.semaphore_signal(
                ready.at[z - early_count], inc=1, device_id={"ep": s}, device_id_type=MESH
            )

    small = [
        pltpu.make_async_copy(source, target, small_sem.at[i])
        for i, (source, target) in enumerate(
            [(tok_hbm, tok), (routes_hbm, routes), (weights_hbm, weights), (gain_hbm, gain)]
        )
    ]
    for copy in small:
        copy.start()
    small[0].wait()
    small[1].wait()
    place = lax.broadcasted_iota(jnp.int32, (all_rows, tok_rows), 0)
    place_expert = lax.div(place, cap)
    place_turn = lax.rem(place, cap)
    hits = [
        (jnp.broadcast_to(routes[k : k + 1, :], (all_rows, tok_rows)) == place_expert)
        for k in range(top)
    ]
    member = sum(hit.astype(jnp.float32) for hit in hits)
    earlier = (
        lax.broadcasted_iota(jnp.int32, (tok_rows, tok_rows), 0)
        < lax.broadcasted_iota(jnp.int32, (tok_rows, tok_rows), 1)
    ).astype(jnp.float32).astype(jnp.bfloat16)
    turn = jnp.dot(member.astype(jnp.bfloat16), earlier, preferred_element_type=jnp.float32)
    chosen = jnp.where(turn == place_turn.astype(jnp.float32), member, 0.0)
    outbox = jnp.dot(
        chosen.astype(jnp.bfloat16), tok[...], preferred_element_type=jnp.float32
    ).astype(jnp.bfloat16)
    packed[...] = outbox.reshape(n_ep, cap, width)

    @pl.when(z < early_count)
    def _():
        pl.semaphore_wait(barrier, early_count - 1 + CHIPS)

    def send(src, dst, send_sem, recv_sem, device):
        copy = pltpu.make_async_remote_copy(
            src_ref=src, dst_ref=dst, send_sem=send_sem, recv_sem=recv_sem,
            device_id=device, device_id_type=MESH,
        )
        copy.start()
        return copy

    def landed(ref, semaphore):
        pltpu.make_async_copy(ref, ref, semaphore).wait()

    def place_rows(i):
        return pl.ds(pl.multiple_of(i * cap, cap), cap)

    my_place = sum(
        ORDER.index(s) * (1 - (lax.rem(z - s + n_ep, n_ep) + n_ep - 1) // n_ep)
        for s in range(n_ep)
    )

    def dispatch(s):
        return pltpu.make_async_remote_copy(
            src_ref=packed.at[s], dst_ref=gathered.at[0, 0, place_rows(my_place), :],
            send_sem=z_send, recv_sem=z_recv.at[z],
            device_id={"ep": s}, device_id_type=MESH,
        )

    for offset in far_offsets:
        s = lax.rem(z + offset, n_ep)

        @pl.when((z >= early_count) | (s < early_count))
        def _():
            dispatch(s).start()

    def dispatch_late(s):
        @pl.when(z < early_count)
        def _():
            pl.semaphore_wait(ready.at[s - early_count], 1)
            dispatch(s).start()

    gathered[0, 0, place_rows(my_place), :] = packed[z]

    for p in range(2):
        for d in range(CHIPS):
            first = pl.multiple_of(owner(p, d) * width, width)
            k = p * CHIPS + d
            for j, source in enumerate((wg_hbm, wu_hbm)):
                pltpu.make_async_copy(
                    source.at[0, pl.ds(first, width), :],
                    w_in.at[pl.ds(k * width, width), pl.ds(j * hidden_units, hidden_units)],
                    in_sem,
                ).start()
    for p, target, sem in ((1, w_other, other_sem), (0, w_own, own_sem)):
        for d in range(CHIPS):
            first = pl.multiple_of(owner(p, d) * width, width)
            pltpu.make_async_copy(
                wd_hbm.at[0, :, pl.ds(first, width)], target.at[:, pl.ds(d * width, width)], sem
            ).start()

    small[2].wait()
    mix = sum(
        jnp.where(hit, jnp.broadcast_to(weights[k : k + 1, :], (all_rows, tok_rows)), 0.0)
        for k, hit in enumerate(hits)
    ) * chosen
    mix_high = mix.astype(jnp.bfloat16)
    mix_low = (mix - mix_high.astype(jnp.float32)).astype(jnp.bfloat16)
    unit = (
        lax.broadcasted_iota(jnp.int32, (tok_rows, tok_rows), 0)
        == lax.broadcasted_iota(jnp.int32, (tok_rows, tok_rows), 1)
    ).astype(jnp.float32).astype(jnp.bfloat16)

    def flipped(value):
        return lax.dot_general(
            unit, value, (((1,), (1,)), ((), ())), preferred_element_type=jnp.float32
        ).astype(jnp.bfloat16)

    mix_high, mix_low = flipped(mix_high), flipped(mix_low)

    def span(c):
        return pl.ds(firsts[c], firsts[c + 1] - firsts[c])

    def halved(c):
        return ((CUTS[c + 1] - CUTS[c] + 1) // 2) * cap

    def top_half(c):
        return pl.ds(firsts[c], halved(c))

    def low_half(c):
        return pl.ds(firsts[c] + halved(c), firsts[c + 1] - firsts[c] - halved(c))

    ag, d2d, halves = {}, {}, {}

    def to_sibling(c, d, at, kind):
        d2d[c, kind] = send(
            gathered.at[0, d, at, :], gathered.at[1, d, at, :],
            d2d_send.at[c], d2d_recv.at[c, kind], sibling,
        )

    def gather_own(c):
        for i in range(CUTS[c], CUTS[c + 1]):

            @pl.when(ORDER[i] != z)
            def _():
                landed(gathered.at[0, 0, place_rows(i), :], z_recv.at[ORDER[i]])

        if c in DIRECT:
            hops = [(CHIPS - d, d) for d in far_first]
        else:
            hops = [(2, 6), (6, 2), (1, 7), (7, 1)]
        for slot, d in hops:
            ag[c, slot] = send(
                gathered.at[0, 0, span(c), :], gathered.at[0, slot, span(c), :],
                ag_send.at[c], ag_recv.at[c, slot], at_chip(d),
            )
        to_sibling(c, 0, span(c), 0)

    def share(c):
        for slot in (1, 7, 2, 6, 3, 5, 4):
            ag[c, slot].wait_recv()
            to_sibling(c, slot, span(c), slot)

    def gather_relay(c):
        for slot, near, far, opposite, at, kind in (
            (2, 7, 6, 3, top_half(c), 4),
            (6, 1, 2, 5, low_half(c), 0),
        ):
            ag[c, slot].wait_recv()
            ag[c, kind] = send(
                gathered.at[0, slot, at, :], gathered.at[0, 4, at, :],
                ag_send.at[c], ag_recv.at[c, kind], at_chip(far),
            )
            ag[c, opposite] = send(
                gathered.at[0, slot, span(c), :], gathered.at[0, opposite, span(c), :],
                ag_send.at[c], ag_recv.at[c, opposite], at_chip(near),
            )
            to_sibling(c, slot, span(c), slot)
        for slot in (1, 7):
            ag[c, slot].wait_recv()
            to_sibling(c, slot, span(c), slot)

    def gather_last(c):
        for slot in (3, 5):
            ag[c, slot].wait_recv()
            to_sibling(c, slot, span(c), slot)
        ag[c, 4].wait_recv()
        to_sibling(c, 4, top_half(c), 4)
        ag[c, 0].wait_recv()
        to_sibling(c, 4, low_half(c), 8)

    def feed(c):
        for kind in range(8 if c in DIRECT else 9):
            d2d[c, kind].wait_recv()
        blocks = [(p, d) for p in range(2) for d in range(CHIPS)]
        features = len(blocks) * width
        shape = (firsts[c + 1] - firsts[c], width)
        total = jnp.zeros(shape, jnp.float32)
        for p, d in blocks:
            total += gathered[p, d, span(c), :].astype(jnp.float32)
        average = jnp.sum(total, axis=1, keepdims=True) / features
        total = jnp.zeros(shape, jnp.float32)
        for p, d in blocks:
            off = gathered[p, d, span(c), :].astype(jnp.float32) - average
            total += off * off
        scale = lax.rsqrt(jnp.sum(total, axis=1, keepdims=True) / features + epsilon)
        for p, d in blocks:
            k = p * CHIPS + d
            off = gathered[p, d, span(c), :].astype(jnp.float32) - average
            rows_in[span(c), pl.ds(k * width, width)] = (
                off * scale * gain[pl.ds(owner(p, d), 1), :]
            ).astype(jnp.bfloat16)

    def expert(c):
        both = jnp.dot(rows_in[span(c), :], w_in[...], preferred_element_type=jnp.float32)
        gate_val, up_val = both[:, :hidden_units], both[:, hidden_units:]
        return (gate_val / (1.0 + jnp.exp(-gate_val)) * up_val).astype(jnp.bfloat16)

    def project(c, hidden):
        other = jnp.dot(hidden, w_other[...], preferred_element_type=jnp.float32)
        other = other.astype(jnp.bfloat16)
        for d in range(CHIPS):
            part_out[d, span(c), :] = other[:, d * width : (d + 1) * width]
        halves[c] = send(
            part_out.at[:, span(c), :], part_in.at[:, span(c), :],
            half_send.at[c], half_recv.at[c], sibling,
        )
        own = jnp.dot(hidden, w_own[...], preferred_element_type=jnp.float32)
        for d in range(CHIPS):
            part_own[d, span(c), :] = own[:, d * width : (d + 1) * width]

    def serve(c):
        feed(c)
        project(c, expert(c))

    def chip_part(d, at):
        return part_own[d, at, :] + part_in[d, at, :].astype(jnp.float32)

    def reduce_send(c, kind, d, source, slot, at):
        send(
            sums_out.at[source, at, :], sums_in.at[slot, at, :],
            rs_send.at[c], rs_recv.at[c, kind], at_chip(d),
        )

    def reduced(c, kind, at):
        landed(sums_in.at[kind or 4, at, :], rs_recv.at[c, kind])

    def reduce_direct(c):
        halves[c].wait_recv()
        for d in far_first:
            sums_out[d, span(c), :] = chip_part(d, span(c)).astype(jnp.bfloat16)
            reduce_send(c, CHIPS - d, d, d, CHIPS - d, span(c))

    def finish_direct(c):
        value = chip_part(0, span(c))
        for slot in far_first:
            reduced(c, slot, span(c))
            value += sums_in[slot, span(c), :].astype(jnp.float32)
        give_back(c, value)

    def reduce_first(c):
        halves[c].wait_recv()
        sums_out[4, span(c), :] = chip_part(4, span(c)).astype(jnp.bfloat16)
        reduce_send(c, 4, 2, 4, 4, top_half(c))
        reduce_send(c, 0, 6, 4, 4, low_half(c))
        for d, near in ((3, 1), (5, 7), (1, 1), (7, 7)):
            sums_out[d, span(c), :] = chip_part(d, span(c)).astype(jnp.bfloat16)
            reduce_send(c, d, near, d, d, span(c))

    def reduce_second(c):
        reduced(c, 4, top_half(c))
        reduced(c, 0, low_half(c))
        for d, near, joined, alone in (
            (2, 3, top_half(c), low_half(c)), (6, 5, low_half(c), top_half(c))
        ):
            reduced(c, near, span(c))
            sums_out[d, joined, :] = (
                chip_part(d, joined)
                + sums_in[near, joined, :].astype(jnp.float32)
                + sums_in[4, joined, :].astype(jnp.float32)
            ).astype(jnp.bfloat16)
            sums_out[d, alone, :] = (
                chip_part(d, alone) + sums_in[near, alone, :].astype(jnp.float32)
            ).astype(jnp.bfloat16)
            reduce_send(c, d, d, d, d, span(c))

    def finish(c):
        value = chip_part(0, span(c))
        for slot in (1, 7, 2, 6):
            reduced(c, slot, span(c))
            value += sums_in[slot, span(c), :].astype(jnp.float32)
        give_back(c, value)

    def back(i):
        return pltpu.make_async_remote_copy(
            src_ref=served.at[place_rows(i), :], dst_ref=returned.at[z],
            send_sem=back_send, recv_sem=back_recv.at[z],
            device_id={"ep": ORDER[i]}, device_id_type=MESH,
        )

    def give_back(c, value):
        served[span(c), :] = value.astype(jnp.bfloat16)
        for i in range(CUTS[c], CUTS[c + 1]):

            @pl.when(ORDER[i] != z)
            def _():
                back(i).start()

            @pl.when(ORDER[i] == z)
            def _():
                returned[z] = served[place_rows(i), :]

    gather_own(0)
    for s in range(n_ep - 1, early_count - 1, -1):
        dispatch_late(s)
    gather_own(1)
    share(0)
    gather_own(2)
    small[3].wait()
    pltpu.make_async_copy(w_in, w_in, in_sem).wait()
    pltpu.make_async_copy(w_other, w_other, other_sem).wait()
    pltpu.make_async_copy(w_own, w_own, own_sem).wait()
    serve(0)
    gather_relay(1)
    reduce_direct(0)
    gather_relay(2)
    gather_last(1)
    serve(1)
    finish_direct(0)
    gather_last(2)
    reduce_first(1)
    serve(2)
    reduce_first(2)
    reduce_second(1)
    reduce_second(2)
    finish(1)
    finish(2)

    landed(packed.at[1:], z_send)
    for c in range(CHUNKS):
        landed(gathered.at[0, 1:, span(c), :], ag_send.at[c])
        landed(gathered.at[0, :, span(c), :], d2d_send.at[c])
        landed(part_out.at[:, span(c), :], half_send.at[c])
        landed(sums_out.at[1:, span(c), :], rs_send.at[c])
    for e in range(n_ep):

        @pl.when(e != z)
        def _():
            landed(returned.at[e], back_recv.at[e])

    values = returned[...].reshape(all_rows, width)
    out_ref[...] = (
        jnp.dot(mix_high, values, preferred_element_type=jnp.float32)
        + jnp.dot(mix_low, values, preferred_element_type=jnp.float32)
    ).astype(out_ref.dtype)
    landed(served.at[pl.ds(cap, all_rows - cap), :], back_send)


def solution(mesh):
    n_ep, n_tp = mesh.shape["ep"], mesh.shape["tp"]

    def on_device(tokens, gain, routes, weights, w_gate, w_up, w_down):
        tok_rows, width = tokens.shape
        top = routes.shape[1]
        cap = min(tok_rows, 2 * tok_rows * top // n_ep)
        hidden_units = w_gate.shape[2]
        all_rows = n_ep * cap
        features = n_tp * width
        bf16, f32 = jnp.bfloat16, jnp.float32
        dma = pltpu.SemaphoreType.DMA
        return pl.pallas_call(
            functools.partial(kernel, n_ep, cap),
            out_shape=pltpu.VMEM((tok_rows, width), bf16),
            in_specs=[pl.BlockSpec(memory_space=pltpu.HBM)] * 7,
            out_specs=pl.BlockSpec(memory_space=pltpu.VMEM),
            scratch_shapes=[
                pltpu.VMEM((tok_rows, width), bf16),
                pltpu.VMEM((n_tp, width), f32),
                pltpu.VMEM((top, tok_rows), jnp.int32),
                pltpu.VMEM((top, tok_rows), f32),
                pltpu.VMEM((features, 2 * hidden_units), bf16),
                pltpu.VMEM((hidden_units, features // 2), bf16),
                pltpu.VMEM((hidden_units, features // 2), bf16),
                pltpu.VMEM((n_ep, cap, width), bf16),
                pltpu.VMEM((2, CHIPS, all_rows, width), bf16),
                pltpu.VMEM((all_rows, features), bf16),
                pltpu.VMEM((CHIPS, all_rows, width), f32),
                pltpu.VMEM((CHIPS, all_rows, width), bf16),
                pltpu.VMEM((CHIPS, all_rows, width), bf16),
                pltpu.VMEM((CHIPS, all_rows, width), bf16),
                pltpu.VMEM((CHIPS, all_rows, width), bf16),
                pltpu.VMEM((all_rows, width), bf16),
                pltpu.VMEM((n_ep, cap, width), bf16),
                dma((4,)), dma, dma, dma, pltpu.SemaphoreType.REGULAR((LATE,)),
                dma, dma((n_ep,)),
                dma((CHUNKS,)), dma((CHUNKS, 8)),
                dma((CHUNKS,)), dma((CHUNKS, 9)),
                dma((CHUNKS,)), dma((CHUNKS,)),
                dma((CHUNKS,)), dma((CHUNKS, 8)),
                dma, dma((n_ep,)),
            ],
            compiler_params=pltpu.CompilerParams(collective_id=0, has_side_effects=True),
        )(tokens, gain.reshape(n_tp, width), routes.T, weights.T, w_gate, w_up, w_down)

    in_specs = (
        P(("grp", "ep"), "tp"),
        P(),
        P(("grp", "ep"), None),
        P(("grp", "ep"), None),
        P("ep", None, "tp"),
        P("ep", None, "tp"),
        P("ep", "tp", None),
    )
    out_specs = P(("grp", "ep"), "tp")
    return jax.shard_map(
        on_device, mesh=mesh, in_specs=in_specs, out_specs=out_specs, check_vma=False
    )
```
